256 devices in a mesh: sp: 32 (over z, x), tp: 8 (over y, core).
Axes of the slice: x: 4, y: 4, z: 8, core: 2. Of those that a mesh axis runs over, the one named last changes fastest.
Arguments:
- latents: bfloat16 [16384, 2048], P(('sp', 'tp')), may hold values from -6 to 6
- context: bfloat16 [512, 2048], P('sp'), may hold values from -6 to 6
- cond: float32 [2048], P('sp'), may hold values from -6 to 6
- ctx_cond: float32 [2048], P('sp'), may hold values from -6 to 6
- mod_weight: float32 [2048, 6144], P('sp', 'tp'), may hold values from -0.125 to 0.125
- query_weight: bfloat16 [2048, 2048], P(None, 'tp'), may hold values from -1 to 1, as said below
- key_matrix: bfloat16 [2048, 1024], P(None, 'tp'), may hold values from -1 to 1, as said below
- value_matrix: bfloat16 [2048, 1024], P(None, 'tp'), may hold values from -0.125 to 0.125
- out_weight: bfloat16 [2048, 2048], P('tp'), may hold values from -0.125 to 0.125
- query_gain: float32 [128], replicated, may hold values from 0.7 to 7
- key_gain: float32 [128], replicated, may hold values from 0.7 to 7
Outputs:
- updated: bfloat16 [16384, 2048], P(('sp', 'tp'))
The draws below stay inside these ranges and needn't reach their ends.
Inputs may be any that keep to these rules, and one draw needn't show every extreme that they name: `query_weight`: entries of order 2048 to the power -1/2. `key_matrix`: entries of order 2048 to the power -1/2.
All inputs are finite; a program needn't handle non-finite values.
Results may differ from the reference program's by a relative error of at most 0.0085.
The reference program's roundings to bfloat16 on the way count: a program that leaves them out, or rounds other values in their place, can miss the bound.
Values may be sent and summed in bfloat16 or wider, within the bound.
A program may use at most 128 MiB of HBM per device.

```python
import math
import jax
import jax.numpy as jnp
from jax import lax

MODEL_DIM = 2048
HEAD_SIZE = 128
QUERY_HEAD_COUNT = 16
KEY_VALUE_HEADS = 8
GRID_W = 64
CTX = 512
TOKENS = 16384


def paired_weights(key):
    query_base = jax.random.normal(jax.random.fold_in(key, 11), (MODEL_DIM, QUERY_HEAD_COUNT * HEAD_SIZE), jnp.float32) * MODEL_DIM ** (-0.5)
    key_start = jax.random.normal(jax.random.fold_in(key, 12), (MODEL_DIM, KEY_VALUE_HEADS * HEAD_SIZE), jnp.float32) * MODEL_DIM ** (-0.5)
    return (query_base, key_start)


def draw_query_weight(key, part):
    return paired_weights(key)[0].astype(jnp.bfloat16)


def draw_key_matrix(key, part):
    return paired_weights(key)[1].astype(jnp.bfloat16)


def draw_query_gain(key, part):
    return jax.random.uniform(jax.random.fold_in(key, 21), (HEAD_SIZE,), jnp.float32, 0.7, 1.3)


def draw_key_gain(key, part):
    return jax.random.uniform(jax.random.fold_in(key, 22), (HEAD_SIZE,), jnp.float32, 0.7, 1.3)


def shard_levels(rng, dims, shards, smallest, high):
    loudness, own = 1.0, jax.random.fold_in(rng, 6)
    for position, parts in shards:
        draws = jnp.exp(jax.random.uniform(jax.random.fold_in(own, position), (parts,), jnp.float32, smallest / len(shards), high / len(shards)))
        loudness = loudness * jnp.repeat(draws, dims[position] // parts).reshape([-1 if axis == position else 1 for axis in range(len(dims))])
    return loudness


def centred(stream_key, dims, width, most, pieces=(), kind=jnp.bfloat16):
    result = jax.random.normal(stream_key, dims, jnp.float32) * width
    if len(pieces) > 0:
        result = shard_levels(stream_key, dims, pieces, -0.22, 0.18) * result
    return jnp.clip(result, min=-most, max=most).astype(kind)


def setup_inputs(seed: int = 0) -> dict:
    key_of = jax.random.split(jax.random.key(seed), 12)
    latents = centred(key_of[0], (TOKENS, MODEL_DIM), 1.0, 6.0, ((0, 256),))
    context = centred(key_of[1], (CTX, MODEL_DIM), 1.0, 6.0, ((0, 32),))
    cond = centred(key_of[2], (MODEL_DIM,), 1.0, 6.0, ((0, 32),), jnp.float32)
    ctx_cond = centred(key_of[3], (MODEL_DIM,), 1.0, 6.0, ((0, 32),), jnp.float32)
    mod_weight = centred(key_of[4], (MODEL_DIM, 3 * MODEL_DIM), MODEL_DIM ** -0.5, 0.125, ((0, 32), (1, 8)), jnp.float32)
    query_weight = draw_query_weight(jax.random.fold_in(key_of[11], 71), 0)
    key_matrix = draw_key_matrix(jax.random.fold_in(key_of[11], 71), 0)
    value_matrix = centred(key_of[7], (MODEL_DIM, KEY_VALUE_HEADS * HEAD_SIZE), MODEL_DIM ** -0.5, 0.125, ((1, 8),))
    out_weight = centred(key_of[8], (QUERY_HEAD_COUNT * HEAD_SIZE, MODEL_DIM), (QUERY_HEAD_COUNT * HEAD_SIZE) ** -0.5, 0.125, ((0, 8),))
    query_gain = draw_query_gain(jax.random.fold_in(key_of[11], 71), 0)
    key_gain = draw_key_gain(jax.random.fold_in(key_of[11], 71), 0)
    return {"latents": latents, "context": context, "cond": cond, "ctx_cond": ctx_cond, "mod_weight": mod_weight, "query_weight": query_weight, "key_matrix": key_matrix, "value_matrix": value_matrix, "out_weight": out_weight, "query_gain": query_gain, "key_gain": key_gain}


NORM_EPS = 1e-06
ROPE_BASE = 10000.0

def normalize(latent_value_rows):
    return latent_value_rows * lax.rsqrt(lax.optimization_barrier(jnp.mean(latent_value_rows * latent_value_rows, axis=-1, keepdims=True)) + NORM_EPS)

def rotate(latent_value_rows, positions):
    quarter = latent_value_rows.shape[-1] // 2
    inv_freq = ROPE_BASE ** (-jnp.arange(quarter, dtype=jnp.float32) / quarter)
    angles = positions.astype(jnp.float32)[:, None] * inv_freq[None, :]
    cos_table = jnp.cos(angles)[:, None, :]
    sin_table = jnp.sin(angles)[:, None, :]
    first, second = (latent_value_rows[..., :quarter], latent_value_rows[..., quarter:])
    return jnp.concatenate([first * cos_table - second * sin_table, second * cos_table + first * sin_table], axis=-1)

def axial(latent_value_rows, positions):
    half_dim = latent_value_rows.shape[-1] // 2
    return jnp.concatenate([rotate(latent_value_rows[..., :half_dim], positions // GRID_W), rotate(latent_value_rows[..., half_dim:], positions % GRID_W)], axis=-1)

def modulate(latent_value_rows, mod_row):
    model_width = latent_value_rows.shape[-1]
    shift_vec = mod_row[:model_width]
    scale_vec = mod_row[model_width:2 * model_width]
    return (normalize(latent_value_rows.astype(jnp.float32)) * (1.0 + scale_vec) + shift_vec).astype(jnp.bfloat16)

def reference(latents, context, cond, ctx_cond, mod_weight, query_weight, key_matrix, value_matrix, out_weight, query_gain, key_gain):
    model_width = latents.shape[1]
    latent_count = latents.shape[0]
    prefix_count = context.shape[0]
    modulation = jnp.dot(jax.nn.silu(jnp.stack([cond, ctx_cond])), mod_weight, precision=lax.Precision.HIGHEST)
    gate_vec = modulation[0, 2 * model_width:]
    normalised_rows = modulate(latents, modulation[0])
    prefix_normalised = modulate(context, modulation[1])
    positions = jnp.arange(latent_count, dtype=jnp.int32)
    query_rows = jnp.dot(normalised_rows, query_weight, preferred_element_type=jnp.float32).reshape(latent_count, QUERY_HEAD_COUNT, HEAD_SIZE)
    query_rows = axial(normalize(query_rows) * query_gain, positions).astype(jnp.bfloat16)
    latent_key_rows = jnp.dot(normalised_rows, key_matrix, preferred_element_type=jnp.float32).reshape(latent_count, KEY_VALUE_HEADS, HEAD_SIZE)
    latent_key_rows = axial(normalize(latent_key_rows) * key_gain, positions).astype(jnp.bfloat16)
    latent_value_rows = jnp.dot(normalised_rows, value_matrix, preferred_element_type=jnp.float32).reshape(latent_count, KEY_VALUE_HEADS, HEAD_SIZE).astype(jnp.bfloat16)
    prefix_keys = jnp.dot(prefix_normalised, key_matrix, preferred_element_type=jnp.float32).reshape(prefix_count, KEY_VALUE_HEADS, HEAD_SIZE)
    prefix_keys = (normalize(prefix_keys) * key_gain).astype(jnp.bfloat16)
    prefix_values = jnp.dot(prefix_normalised, value_matrix, preferred_element_type=jnp.float32).reshape(prefix_count, KEY_VALUE_HEADS, HEAD_SIZE).astype(jnp.bfloat16)
    keys_all = jnp.concatenate([prefix_keys, latent_key_rows], axis=0).astype(jnp.float32)
    values_all = jnp.concatenate([prefix_values, latent_value_rows], axis=0).astype(jnp.float32)
    lift = math.log(latent_count / (2.0 * prefix_count))
    lift_row = jnp.concatenate([jnp.full((prefix_count,), lift, jnp.float32), jnp.zeros((latent_count,), jnp.float32)])
    group_size = QUERY_HEAD_COUNT // KEY_VALUE_HEADS
    rows_per_block = math.gcd(latent_count, 256)
    token_blocks = query_rows.reshape(latent_count // rows_per_block, rows_per_block, KEY_VALUE_HEADS, group_size, HEAD_SIZE)
    inv_root = HEAD_SIZE ** (-0.5)

    def one_block(block):
        scores = jnp.einsum('qhgd,khd->hgqk', block.astype(jnp.float32), keys_all) * inv_root + lift_row
        top_row = lax.optimization_barrier(jnp.max(scores, axis=-1, keepdims=True))
        weights = jnp.exp(scores - top_row)
        total = lax.optimization_barrier(jnp.sum(weights, axis=-1))
        probs = lax.optimization_barrier(weights.astype(jnp.bfloat16)).astype(jnp.float32)
        summed = jnp.einsum('hgqk,khd->qhgd', probs, values_all)
        return (summed / jnp.transpose(total, (2, 0, 1))[..., None]).astype(jnp.bfloat16)
    attended = lax.map(one_block, token_blocks).reshape(latent_count, QUERY_HEAD_COUNT * HEAD_SIZE)
    mixed = jnp.dot(attended, out_weight, preferred_element_type=jnp.float32)
    return (latents.astype(jnp.float32) + gate_vec * normalize(mixed)).astype(jnp.bfloat16)
```

```python
import functools
import math

import jax
import jax.numpy as jnp
from jax import lax
from jax.experimental import pallas as pl
from jax.experimental.pallas import tpu as pltpu
from jax.sharding import PartitionSpec as P

GRID_W = 64
NORM_EPS = 1e-06
ROPE_BASE = 10000.0
MESH = pl.DeviceIdType.MESH
BF16 = jnp.bfloat16
F32 = jnp.float32
VMEM_BYTES = 67043328


def row_size(sp_count):
    size = 1
    while 4 * size * size <= sp_count:
        size *= 2
    return size


def tables(positions, head_dim):
    quarter = head_dim // 4
    inv_freq = ROPE_BASE ** (-jnp.arange(quarter, dtype=F32) / quarter)
    where = jnp.stack([positions // GRID_W, positions % GRID_W]).astype(F32)
    angles = where[:, None, :] * inv_freq[None, :, None]
    return jnp.cos(angles), jnp.sin(angles)


def remote(src, dst, send, recv, dev):
    return pltpu.make_async_remote_copy(
        src_ref=src, dst_ref=dst, send_sem=send, recv_sem=recv, device_id=dev, device_id_type=MESH
    )


def front_kernel(
    sp_count, tp_count, x_count, head_dim,
    cond_ref, cond_1_ref, mw_hbm, lat_hbm, ctx_ref, wq_hbm, wk_hbm, wv_hbm, qg_ref, kg_ref, cos_ref, sin_ref,
    qb, kb, vb, cb, gate_ref, q_send, q_recv, kv_send, kv_recv, c_send, c_recv,
    mw, lat, wq, wk, wv, part, tot, mod, xn, load_sem,
    lat_send, lat_recv, pair_send, pair_recv, part_send, part_recv, tot_send, tot_recv,
    wo_hbm, wo_vm, wo_sem,
):
    s, t = lax.axis_index("sp"), lax.axis_index("tp")
    y, c = t // 2, t % 2
    z, x = s // x_count, s % x_count
    z_count = sp_count // x_count
    y_count = tp_count // 2
    partner = y * 2 + 1 - c
    rows = lat.shape[1]
    half = rows // 2
    width = lat.shape[2]
    model_cols = mod.shape[1]
    right, left, far = [((y + j) % y_count) * 2 + c for j in (1, y_count - 1, 2)]

    own = pltpu.make_async_copy(lat_hbm, lat.at[t], load_sem.at[0])
    own.start()
    loads = [
        pltpu.make_async_copy(a, b, load_sem.at[1 + i])
        for i, (a, b) in enumerate(((mw_hbm, mw), (wq_hbm, wq), (wk_hbm, wk), (wv_hbm, wv)))
    ]
    for one in loads:
        one.start()
    pltpu.make_async_copy(wo_hbm, wo_vm, wo_sem.at[0]).start()

    barrier = pltpu.get_barrier_semaphore()
    for j in range(1, sp_count):
        pl.semaphore_signal(barrier, inc=1, device_id=((s + j) % sp_count, t), device_id_type=MESH)
    for j in range(1, tp_count):
        pl.semaphore_signal(barrier, inc=1, device_id=(s, (t + j) % tp_count), device_id_type=MESH)

    loads[0].wait()
    lines = lax.broadcasted_iota(jnp.int32, (8, cond_ref.shape[1]), 0)
    cond = jnp.where(lines == 0, cond_ref[...], jnp.where(lines == 1, cond_1_ref[...], 0.0))
    cond = cond * jax.nn.sigmoid(cond)
    part[s] = jnp.dot(
        cond, mw[...], precision=lax.Precision.HIGHEST, preferred_element_type=F32
    )[:2]
    own.wait()
    pl.semaphore_wait(barrier, sp_count + tp_count - 2)

    started = []

    def go(one):
        one.start()
        started.append(one)

    def lat_half(src, n, send, dev):
        at = pl.ds(n * half, half)
        return remote(
            lat.at[src, at], lat.at[src, at], lat_send.at[send], lat_recv.at[src, n], (s, dev)
        )

    def pair(src, send):
        return remote(lat.at[src], lat.at[src], pair_send.at[send], pair_recv.at[src], (s, partner))

    for j in range(1, sp_count):
        go(remote(part.at[s], part.at[s], part_send.at[j], part_recv.at[s], ((s + j) % sp_count, t)))
    go(lat_half(t, 0, 0, right))
    go(lat_half(t, 1, 1, left))
    go(lat_half(t, 1, 2, right))
    go(lat_half(t, 0, 3, left))
    go(pair(t, 0))

    total = part[s]
    for j in range(1, sp_count):
        src = (s + j) % sp_count
        remote(part.at[src], part.at[src], part_send.at[0], part_recv.at[src], (s, t)).wait_recv()
    total = part[0]
    for j in range(1, sp_count):
        total = total + part[j]
    tot[t] = total
    for j in range(1, tp_count):
        go(remote(tot.at[t], tot.at[t], tot_send.at[j], tot_recv.at[t], (s, (t + j) % tp_count)))

    lat_half(left, 0, 0, t).wait_recv()
    go(lat_half(left, 0, 4, right))
    lat_half(right, 1, 0, t).wait_recv()
    go(lat_half(right, 1, 5, left))
    lat_half(left, 1, 0, t).wait_recv()
    go(pair(left, 1))
    lat_half(right, 0, 0, t).wait_recv()
    go(pair(right, 2))

    for j in range(1, tp_count):
        src = (t + j) % tp_count
        remote(tot.at[src], tot.at[src], tot_send.at[0], tot_recv.at[src], (s, t)).wait_recv()
    cols = model_cols // tp_count
    for j in range(tp_count):
        mod[:, j * cols : (j + 1) * cols] = tot[j]
    gate_ref[...] = mod[0:1, 2 * width :]

    def modulate(x_rows, r):
        x_rows = x_rows.astype(F32)
        scaled = x_rows * lax.rsqrt(jnp.mean(x_rows * x_rows, axis=-1, keepdims=True) + NORM_EPS)
        shift, scale = mod[r : r + 1, :width], mod[r : r + 1, width : 2 * width]
        return (scaled * (1.0 + scale) + shift).astype(BF16)

    for one in loads[1:]:
        one.wait()

    q4 = head_dim // 4
    qgain, kgain = qg_ref[...], kg_ref[...]

    def turn(yt, cos, sin):
        out = []
        for n in range(2):
            a = yt[2 * n * q4 : (2 * n + 1) * q4]
            b = yt[(2 * n + 1) * q4 : (2 * n + 2) * q4]
            out += [a * cos[n] - b * sin[n], b * cos[n] + a * sin[n]]
        return jnp.concatenate(out, axis=0)

    def unit(yh, gain):
        return yh * lax.rsqrt(jnp.mean(yh * yh, axis=-1, keepdims=True) + NORM_EPS) * gain

    span = 2 * rows

    def block(j, yy):
        for i in range(2):
            xn[i * rows : (i + 1) * rows, :] = modulate(lat[yy * 2 + i], 0)
        xb = xn[...]
        at = pl.ds(pl.multiple_of(yy * span, span), span)
        cos, sin = cos_ref[:, :, at], sin_ref[:, :, at]
        key = jnp.dot(xb, wk[...], preferred_element_type=F32)
        val = jnp.dot(xb, wv[...], preferred_element_type=F32)
        full = jnp.dot(xb, wq[...], preferred_element_type=F32)
        kb[z, j * span : (j + 1) * span, :] = turn(unit(key, kgain).T, cos, sin).T.astype(BF16)
        vb[z, j // 2, :, (j % 2) * span : (j % 2 + 1) * span] = val.T.astype(BF16)
        for h in range(full.shape[1] // head_dim):
            yh = full[:, h * head_dim : (h + 1) * head_dim]
            qb[x, h, :, at] = turn(unit(yh, qgain).T, cos, sin).astype(BF16)
        if j % 2 == 1:
            for way, dz in ((0, 1), (1, z_count - 1)):
                for one in kv_copy(kb, vb, kv_send, kv_recv, z, j // 2, way, ((z + dz) % z_count) * x_count + x, t):
                    go(one)
        for d in (1, x_count - 1):
            go(q_copy(qb, q_send, q_recv, x, yy, j, d, z * x_count + (x + d) % x_count, t))
        return yy

    remote(lat.at[partner], lat.at[partner], pair_send.at[0], pair_recv.at[partner], (s, t)).wait_recv()
    cn = modulate(ctx_ref[...], 1)
    kc = jnp.dot(cn, wk[...], preferred_element_type=F32)
    vc = jnp.dot(cn, wv[...], preferred_element_type=F32)
    cb[z, 0] = unit(kc, kgain).astype(BF16)
    cb[z, 1] = vc.astype(BF16)
    for j in range(1, z_count):
        go(remote(cb.at[z], cb.at[z], c_send.at[j], c_recv.at[z], (((z + j) % z_count) * x_count + x, t)))
    done = [block(0, y)]
    lat_half(far, 0, 0, t).wait_recv()
    lat_half(far, 1, 0, t).wait_recv()
    go(pair(far, 3))
    for j, step in ((1, 1), (2, y_count - 1), (3, 2)):
        yy = (y + step) % y_count
        other = yy * 2 + 1 - c
        remote(lat.at[other], lat.at[other], pair_send.at[0], pair_recv.at[other], (s, t)).wait_recv()
        done.append(block(j, yy))
    for j, yy in enumerate(done):
        go(q_copy(qb, q_send, q_recv, x, yy, j, 2, z * x_count + (x + 2) % x_count, t))
    return started


def kv_copy(kb, vb, kv_send, kv_recv, src, n, way, peer, t, which=(0, 1)):
    half = kb.shape[1] // 2
    both = [
        remote(
            kb.at[src, pl.ds(n * half, half)], kb.at[src, pl.ds(n * half, half)],
            kv_send.at[0, src, way, n], kv_recv.at[0, src, n], (peer, t),
        ),
        remote(
            vb.at[src, n], vb.at[src, n], kv_send.at[1, src, way, n], kv_recv.at[1, src, n], (peer, t)
        ),
    ]
    return [both[i] for i in which]


def q_copy(qb, q_send, q_recv, owner, yy, j, d, peer, t):
    span = qb.shape[3] // 4
    at = pl.ds(pl.multiple_of(yy * span, span), span)
    ref = qb.at[owner, :, :, at]
    return remote(ref, ref, q_send.at[d, j], q_recv.at[owner, yy], (peer, t))


def attend_kernel(
    sp_count, x_count, lift,
    qb, kb, vb, cb, q_send, q_recv, kv_send, kv_recv, c_send, c_recv,
    att, top, tot, acc, ob, ib, om, im, o_send, o_recv, m_send, m_recv, started,
):
    s, t = lax.axis_index("sp"), lax.axis_index("tp")
    z, x = s // x_count, s % x_count
    z_count = sp_count // x_count
    heads, head_dim, rows = qb.shape[1:]
    factor = head_dim ** (-0.5) * math.log2(math.e)
    bias = lift * head_dim**0.5

    top[...] = jnp.full_like(top, -1e30)
    tot[...] = jnp.zeros_like(tot)
    acc[...] = jnp.zeros_like(acc)

    def at_z(k):
        return (z + k + z_count) % z_count

    def soft(d, h, sc, values):
        i = d * heads + h
        old = top[i]
        new = jnp.maximum(old, jnp.max(sc, axis=0, keepdims=True))
        p = jnp.exp2((sc - new) * factor)
        f = jnp.exp2((old - new) * factor)
        top[i] = new
        tot[i] = tot[i] * f + jnp.sum(p, axis=0, keepdims=True)
        p = p.astype(BF16)
        new_acc = acc[i] * f
        step = p.shape[0] // len(values)
        for n, one in enumerate(values):
            new_acc = new_acc + jnp.dot(one, p[n * step : (n + 1) * step], preferred_element_type=F32)
        acc[i] = new_acc

    def units(pairs, with_ctx=None):
        todo = []
        for kv, d in pairs:
            for h in range(heads):
                todo.append((kv, d, h))

        def scores(one):
            kv, d, h = one
            return jnp.dot(kb[kv], qb[(x + d) % x_count, h], preferred_element_type=F32)

        ahead = [scores(one) for one in todo[:2]]
        for n, one in enumerate(todo):
            sc = ahead.pop(0)
            if n + 2 < len(todo):
                ahead.append(scores(todo[n + 2]))
            kv, d, h = one
            soft(d, h, sc, [vb[kv, 0], vb[kv, 1]])

    def arrive(k, sign, which=(0, 1)):
        src = at_z(sign * k)
        for n in range(2):
            for one in kv_copy(kb, vb, kv_send, kv_recv, src, n, 0, s, t, which):
                one.wait_recv()

    def forward(k, which_r=(0, 1), which_l=(0, 1)):
        for n in range(2):
            for sign, way, which in ((-1, 0, which_r), (1, 1, which_l)):
                src = at_z(sign * k)
                for one in kv_copy(kb, vb, kv_send, kv_recv, src, n, 0, s, t):
                    one.wait_recv()
                peer = at_z(1 if way == 0 else -1) * x_count + x
                for one in kv_copy(kb, vb, kv_send, kv_recv, src, n, way, peer, t, which):
                    one.start()
                    started.append(one)

    def q_arrive(d):
        owner = (x + d) % x_count
        for yy in range(4):
            q_copy(qb, q_send, q_recv, owner, yy, 0, 0, s, t).wait_recv()

    units([(z, 0)])
    forward(1)
    q_arrive(x_count - 1)
    q_arrive(1)
    units([(z, 3), (z, 1)])

    def first(i, carry):
        d = jnp.where(i == 0, 3, 2 - i)
        units([(at_z(-1), d), (at_z(1), d)])
        return carry

    lax.fori_loop(0, 3, first, 0)
    forward(2)
    q_arrive(2)
    units([(at_z(-1), 2), (at_z(1), 2)])

    def peers(k):
        def one(i, carry):
            d = jnp.where(i == 2, 1, 2 + i)
            units([(at_z(-k), d), (at_z(k), d)])
            return carry

        lax.fori_loop(0, 3, one, 0)

    peers(2)
    forward(3, (0,), (1,))
    peers(3)
    for j in range(1, z_count):
        src = at_z(j)
        remote(cb.at[src], cb.at[src], c_send.at[0], c_recv.at[src], (s, t)).wait_recv()
    ckeys = jnp.concatenate([cb[j, 0] for j in range(z_count)], axis=0)
    cvals = jnp.concatenate([cb[j, 1] for j in range(z_count)], axis=0).astype(F32).T.astype(BF16)

    def context(d):
        for h in range(heads):
            sc = jnp.dot(ckeys, qb[(x + d) % x_count, h], preferred_element_type=F32) + bias
            soft(d, h, sc, [cvals])

    def give(d):
        peer = z * x_count + (x + d) % x_count
        for h in range(heads):
            i = d * heads + h
            ob[d - 1, h] = (acc[i] / tot[i]).astype(BF16)
            om[d - 1, 2 * h : 2 * h + 1, :] = top[i]
            om[d - 1, 2 * h + 1 : 2 * h + 2, :] = tot[i]
        for a, b, u, v in ((om, im, m_send, m_recv), (ob, ib, o_send, o_recv)):
            one = remote(a.at[d - 1], b.at[d - 1], u.at[d - 1], v.at[d - 1], (peer, t))
            one.start()
            started.append(one)

    for n in range(2):
        for one in kv_copy(kb, vb, kv_send, kv_recv, at_z(4), n, 0, s, t):
            one.wait_recv()
    units([(z, 2), (at_z(4), 2)])
    context(2)
    give(2)
    for d in (3, 1):
        units([(at_z(4), d)])
        context(d)
        give(d)

    def last(k, carry):
        units([(at_z(-k), 0), (at_z(k), 0)])
        return carry

    lax.fori_loop(2, 4, last, 0)
    units([(at_z(4), 0)])
    context(0)
    for d in range(1, x_count):
        for a, b, u, v in ((om, im, m_send, m_recv), (ob, ib, o_send, o_recv)):
            remote(a.at[d - 1], b.at[d - 1], u.at[d - 1], v.at[d - 1], (s, t)).wait_recv()
    for h in range(heads):
        best = top[h]
        for d in range(1, x_count):
            best = jnp.maximum(best, im[d - 1, 2 * h : 2 * h + 1, :])
        f = jnp.exp2((top[h] - best) * factor)
        value, weight = acc[h] * f, tot[h] * f
        for d in range(1, x_count):
            w = im[d - 1, 2 * h + 1 : 2 * h + 2, :] * jnp.exp2(
                (im[d - 1, 2 * h : 2 * h + 1, :] - best) * factor
            )
            value = value + ib[d - 1, h].astype(F32) * w
            weight = weight + w
        att[:, h * head_dim : (h + 1) * head_dim] = (value / weight).T.astype(BF16)


def mix_kernel(
    tp_count, chunks,
    att_ref, wo_hbm, wo_ref, wo_sem, lat_ref, gate_ref,
    out_ref,
    core_out, core_in, mesh_out, mesh_in, mixed, core_send, core_recv, mesh_send, mesh_recv,
):
    s, t = lax.axis_index("sp"), lax.axis_index("tp")
    y, c = t // 2, t % 2
    y_count = tp_count // 2
    partner = y * 2 + 1 - c
    rows, width = lat_ref.shape
    step = width // chunks
    peers = [((y + j) % y_count) * 2 + c for j in range(1, y_count)]
    pltpu.make_async_copy(wo_hbm, wo_ref, wo_sem.at[0]).wait()

    def piece(n, j, cc):
        yy = (y + j) % y_count
        at = pl.ds(pl.multiple_of((yy * 2 + cc) * rows, rows), rows)
        return jnp.dot(
            att_ref[at, :], wo_ref[:, n * step : (n + 1) * step], preferred_element_type=F32
        )

    order = list(range(1, y_count)) + [0]
    cores = [
        remote(core_out.at[n], core_in.at[n], core_send.at[n], core_recv.at[n], (s, partner))
        for n in range(chunks)
    ]
    sent = []
    for n in range(chunks + 1):
        if n < chunks:
            for j in order:
                core_out[n, j] = piece(n, j, 1 - c).astype(BF16)
            cores[n].start()
        if n == 0:
            continue
        m = n - 1
        own = [piece(m, j, c) for j in order]
        cores[m].wait_recv()
        for j, value in zip(order, own):
            value = value + core_in[m, j].astype(F32)
            if j == 0:
                mixed[m] = value
            else:
                mesh_out[m, j - 1] = value.astype(BF16)
                one = remote(
                    mesh_out.at[m, j - 1], mesh_in.at[m, j - 1], mesh_send.at[m, j - 1],
                    mesh_recv.at[m, j - 1], (s, peers[j - 1]),
                )
                one.start()
                sent.append(one)
    for one in sent:
        one.wait_recv()
    square = jnp.zeros((rows, 1), F32)
    for n in range(chunks):
        value = mixed[n]
        for j in range(1, y_count):
            value = value + mesh_in[n, j - 1].astype(F32)
        mixed[n] = value
        square = square + jnp.sum(value * value, axis=-1, keepdims=True)
    inv = lax.rsqrt(square / width + NORM_EPS)
    for n in range(chunks):
        at = slice(n * step, (n + 1) * step)
        out_ref[:, at] = (
            lat_ref[:, at].astype(F32) + gate_ref[:, at] * (mixed[n] * inv)
        ).astype(BF16)
    for one in sent + cores:
        one.wait_send()


def whole_kernel(sp_count, tp_count, x_count, head_dim, lift, chunks, counts, *refs):
    (
        cond, cond_1, mw, lat, ctx, wq, wk, wv, qg, kg, cos, sin, wo, lat_rows,
        out, qb, kb, vb, cb, gate, att, wo_vm, wo_sem, *rest,
    ) = refs
    links, front, middle, last = counts
    ends = [links, links + front, links + front + middle]
    links, front_scratch, middle_scratch = rest[: ends[0]], rest[ends[0] : ends[1]], rest[ends[1] : ends[2]]
    started = front_kernel(
        sp_count, tp_count, x_count, head_dim, cond, cond_1, mw, lat, ctx, wq, wk, wv, qg, kg, cos, sin,
        qb, kb, vb, cb, gate, *links, *front_scratch, wo, wo_vm, wo_sem,
    )
    with jax.named_scope("attn"):
        attend_kernel(
            sp_count, x_count, lift, qb, kb, vb, cb, *links, att, *middle_scratch, started
        )
    with jax.named_scope("mix"):
        mix_kernel(
            tp_count, chunks, att, wo, wo_vm, wo_sem, lat_rows, gate, out, *rest[ends[2] :]
        )
    for one in started:
        one.wait_send()


ANY = pl.BlockSpec(memory_space=pl.ANY)
VM = pl.BlockSpec(memory_space=pltpu.VMEM)
DMA = pltpu.SemaphoreType.DMA


def body(
    latents,
    context,
    cond,
    ctx_cond,
    mod_weight,
    query_weight,
    key_matrix,
    value_matrix,
    out_weight,
    query_gain,
    key_gain,
):
    sp_count, tp_count = lax.axis_size("sp"), lax.axis_size("tp")
    x_count = row_size(sp_count)
    rows, width = latents.shape
    ctx_rows = context.shape[0]
    head_dim = query_gain.shape[0]
    heads = query_weight.shape[1] // head_dim
    all_rows = rows * tp_count
    mod_cols = mod_weight.shape[1]
    positions = lax.axis_index("sp") * all_rows + jnp.arange(all_rows, dtype=jnp.int32)
    cos, sin = tables(positions, head_dim)
    lift = math.log(sp_count * all_rows / (2.0 * sp_count * ctx_rows))
    chunks = 4
    y_count = tp_count // 2
    step = width // chunks
    far = max(y_count - 1, 1)
    z_count = sp_count // x_count
    shared = [
        pltpu.VMEM((x_count, heads, head_dim, all_rows), BF16),
        pltpu.VMEM((z_count, all_rows, head_dim), BF16),
        pltpu.VMEM((z_count, 2, head_dim, all_rows // 2), BF16),
        pltpu.VMEM((z_count, 2, ctx_rows, head_dim), BF16),
        pltpu.VMEM((1, width), F32),
        pltpu.VMEM((all_rows, heads * head_dim), BF16),
        pltpu.VMEM(out_weight.shape, BF16),
        DMA((1,)),
    ]
    links = [
        DMA((x_count, y_count)),
        DMA((x_count, y_count)),
        DMA((2, z_count, 2, 2)),
        DMA((2, z_count, 2)),
        DMA((z_count,)),
        DMA((z_count,)),
    ]
    front = [
        pltpu.VMEM(mod_weight.shape, F32),
        pltpu.VMEM((tp_count, rows, width), BF16),
        pltpu.VMEM(query_weight.shape, BF16),
        pltpu.VMEM(key_matrix.shape, BF16),
        pltpu.VMEM(value_matrix.shape, BF16),
        pltpu.VMEM((sp_count, 2, mod_cols), F32),
        pltpu.VMEM((tp_count, 2, mod_cols), F32),
        pltpu.VMEM((2, mod_cols * tp_count), F32),
        pltpu.VMEM((2 * rows, width), BF16),
        DMA((5,)),
        DMA((6,)),
        DMA((tp_count, 2)),
        DMA((4,)),
        DMA((tp_count,)),
        DMA((sp_count,)),
        DMA((sp_count,)),
        DMA((tp_count,)),
        DMA((tp_count,)),
    ]
    far = x_count - 1
    middle = [
        pltpu.VMEM((x_count * heads, 1, all_rows), F32),
        pltpu.VMEM((x_count * heads, 1, all_rows), F32),
        pltpu.VMEM((x_count * heads, head_dim, all_rows), F32),
        pltpu.VMEM((far, heads, head_dim, all_rows), BF16),
        pltpu.VMEM((far, heads, head_dim, all_rows), BF16),
        pltpu.VMEM((far, 2 * heads, all_rows), F32),
        pltpu.VMEM((far, 2 * heads, all_rows), F32),
        DMA((far,)),
        DMA((far,)),
        DMA((far,)),
        DMA((far,)),
    ]
    far = max(y_count - 1, 1)
    last = [
        pltpu.VMEM((chunks, y_count, rows, step), BF16),
        pltpu.VMEM((chunks, y_count, rows, step), BF16),
        pltpu.VMEM((chunks, far, rows, step), BF16),
        pltpu.VMEM((chunks, far, rows, step), BF16),
        pltpu.VMEM((chunks, rows, step), F32),
        DMA((chunks,)),
        DMA((chunks,)),
        DMA((chunks, far)),
        DMA((chunks, far)),
    ]
    counts = (len(links), len(front), len(middle), len(last))
    return pl.pallas_call(
        functools.partial(
            whole_kernel, sp_count, tp_count, x_count, head_dim, lift, chunks, counts
        ),
        out_shape=jax.ShapeDtypeStruct((rows, width), BF16),
        in_specs=[VM, VM, ANY, ANY, VM, ANY, ANY, ANY, VM, VM, VM, VM, ANY, VM],
        out_specs=VM,
        scratch_shapes=shared + links + front + middle + last,
        compiler_params=pltpu.CompilerParams(
            collective_id=0, has_side_effects=True, vmem_limit_bytes=VMEM_BYTES,
        ),
        name="whole",
    )(
        cond[None], ctx_cond[None], mod_weight, latents, context, query_weight, key_matrix, value_matrix,
        query_gain[None], key_gain[None], cos, sin, out_weight, latents,
    )


def solution(mesh):
    placed = (
        P(("sp", "tp"), None),
        P("sp", None),
        P("sp"),
        P("sp"),
        P("sp", "tp"),
        P(None, "tp"),
        P(None, "tp"),
        P(None, "tp"),
        P("tp", None),
        P(),
        P(),
    )
    return jax.shard_map(
        body, mesh=mesh, in_specs=placed, out_specs=P(("sp", "tp"), None), check_vma=False
    )
```

```python
import functools
import math

import jax
import jax.numpy as jnp
import numpy as np
from jax import lax
from jax.experimental import pallas as pl
from jax.experimental.pallas import tpu as pltpu
from jax.sharding import PartitionSpec as P

GRID_W = 64
NORM_EPS = 1e-06
ROPE_BASE = 10000.0
MESH = pl.DeviceIdType.MESH
BF16 = jnp.bfloat16
F32 = jnp.float32
VMEM_BYTES = 67043328


def row_size(sp_count):
    size = 1
    while 4 * size * size <= sp_count:
        size *= 2
    return size


def remote(src, dst, send, recv, dev):
    return pltpu.make_async_remote_copy(
        src_ref=src, dst_ref=dst, send_sem=send, recv_sem=recv, device_id=dev, device_id_type=MESH
    )


def front_kernel(
    sp_count, tp_count, x_count, head_dim,
    cond_hbm, cond_1_hbm, mw_hbm, lat_hbm, ctx_hbm, wq_hbm, wk_hbm, wv_hbm, qg_hbm, kg_hbm, freq_hbm,
    qb, kb, vb, cb, gate_ref, q_send, q_recv, kv_send, kv_recv, c_send, c_recv,
    mw, lat, wq, wk, wv, part, tot, mod, xn, ctx, cos_ref, sin_ref,
    cond_ref, cond_1_ref, qg_ref, kg_ref, freq_ref, load_sem,
    lat_send, lat_recv, pair_send, pair_recv, part_send, part_recv, tot_send, tot_recv,
    wo_hbm, wo, wo_sem, wo_send, wo_recv, wo_pair_send, wo_pair_recv,
):
    s, t = lax.axis_index("sp"), lax.axis_index("tp")
    y, c = t // 2, t % 2
    z, x = s // x_count, s % x_count
    z_count = sp_count // x_count
    y_count = tp_count // 2
    partner = y * 2 + 1 - c
    rows = lat.shape[1]
    half = rows // 2
    width = lat.shape[2]
    model_cols = mod.shape[1]
    right, left, far = [((y + j) % y_count) * 2 + c for j in (1, y_count - 1, 2)]

    loads = [
        pltpu.make_async_copy(a, b, load_sem.at[i])
        for i, (a, b) in enumerate(
            (
                (cond_hbm, cond_ref), (cond_1_hbm, cond_1_ref), (mw_hbm, mw), (lat_hbm, lat.at[t]),
                (freq_hbm, freq_ref), (kg_hbm, kg_ref), (qg_hbm, qg_ref), (ctx_hbm, ctx),
                (wk_hbm, wk), (wv_hbm, wv), (wq_hbm, wq),
            )
        )
    ]
    for one in loads[:4]:
        one.start()

    barrier = pltpu.get_barrier_semaphore()
    for j in range(1, sp_count):
        pl.semaphore_signal(barrier, inc=1, device_id=((s + j) % sp_count, t), device_id_type=MESH)
    for j in range(1, tp_count):
        pl.semaphore_signal(barrier, inc=1, device_id=(s, (t + j) % tp_count), device_id_type=MESH)

    for one in loads[4:]:
        one.start()
    wo_load = pltpu.make_async_copy(wo_hbm, wo.at[t], wo_sem.at[0])
    wo_load.start()
    for one in loads[:3]:
        one.wait()
    lines = lax.broadcasted_iota(jnp.int32, (8, cond_ref.shape[1]), 0)
    cond = jnp.where(lines == 0, cond_ref[...], jnp.where(lines == 1, cond_1_ref[...], 0.0))
    cond = cond * jax.nn.sigmoid(cond)
    part[s] = jnp.dot(
        cond, mw[...], precision=lax.Precision.HIGHEST, preferred_element_type=F32
    )[:2]
    loads[3].wait()
    with jax.named_scope("barrier"):
        pl.semaphore_wait(barrier, sp_count + tp_count - 2)

    started = []

    def go(one):
        one.start()
        started.append(one)

    def lat_half(src, n, send, dev):
        at = pl.ds(n * half, half)
        return remote(
            lat.at[src, at], lat.at[src, at], lat_send.at[send], lat_recv.at[src, n], (s, dev)
        )

    def pair(src, send):
        return remote(lat.at[src], lat.at[src], pair_send.at[send], pair_recv.at[src], (s, partner))

    for j in range(1, sp_count):
        go(remote(part.at[s], part.at[s], part_send.at[j], part_recv.at[s], ((s + j) % sp_count, t)))
    go(lat_half(t, 0, 0, right))
    go(lat_half(t, 1, 1, left))
    go(lat_half(t, 1, 2, right))
    go(lat_half(t, 0, 3, left))
    go(pair(t, 0))

    loads[4].wait()
    where = s * cos_ref.shape[2] + lax.broadcasted_iota(jnp.int32, cos_ref.shape[1:], 1)
    for n, place in enumerate((where // GRID_W, where % GRID_W)):
        angle = place.astype(F32) * freq_ref[...]
        cos_ref[n] = jnp.cos(angle)
        sin_ref[n] = jnp.sin(angle)

    with jax.named_scope("modsum"):
        total = part[s]
        for j in range(1, sp_count):
            src = (s + j) % sp_count
            remote(part.at[src], part.at[src], part_send.at[0], part_recv.at[src], (s, t)).wait_recv()
        total = part[0]
        for j in range(1, sp_count):
            total = total + part[j]
        tot[t] = total
    for j in range(1, tp_count):
        go(remote(tot.at[t], tot.at[t], tot_send.at[j], tot_recv.at[t], (s, (t + j) % tp_count)))

    with jax.named_scope("latwait"):
        lat_half(left, 0, 0, t).wait_recv()
        go(lat_half(left, 0, 4, right))
        lat_half(right, 1, 0, t).wait_recv()
        go(lat_half(right, 1, 5, left))
        lat_half(left, 1, 0, t).wait_recv()
        go(pair(left, 1))
        lat_half(right, 0, 0, t).wait_recv()
        go(pair(right, 2))

    wo_load.wait()
    for src, n, send, dev in ((t, 0, 0, right), (t, 1, 1, left), (t, 1, 2, right), (t, 0, 3, left)):
        go(wo_half(wo, wo_send, wo_recv, src, n, send, s, dev))
    go(wo_pair(wo, wo_pair_send, wo_pair_recv, t, 0, s, partner))

    with jax.named_scope("totwait"):
        for j in range(1, tp_count):
            src = (t + j) % tp_count
            remote(tot.at[src], tot.at[src], tot_send.at[0], tot_recv.at[src], (s, t)).wait_recv()
    cols = model_cols // tp_count
    for j in range(tp_count):
        mod[:, j * cols : (j + 1) * cols] = tot[j]
    gate_ref[...] = mod[0:1, 2 * width :]

    def modulate(x_rows, r):
        x_rows = x_rows.astype(F32)
        scaled = x_rows * lax.rsqrt(jnp.mean(x_rows * x_rows, axis=-1, keepdims=True) + NORM_EPS)
        shift, scale = mod[r : r + 1, :width], mod[r : r + 1, width : 2 * width]
        return (scaled * (1.0 + scale) + shift).astype(BF16)

    with jax.named_scope("loadwait"):
        for one in loads[5:]:
            one.wait()

    q4 = head_dim // 4
    qgain, kgain = qg_ref[...], kg_ref[...]

    def turn(yt, cos, sin):
        out = []
        for n in range(2):
            a = yt[2 * n * q4 : (2 * n + 1) * q4]
            b = yt[(2 * n + 1) * q4 : (2 * n + 2) * q4]
            out += [a * cos[n] - b * sin[n], b * cos[n] + a * sin[n]]
        return jnp.concatenate(out, axis=0)

    def unit(yh, gain):
        return yh * lax.rsqrt(jnp.mean(yh * yh, axis=-1, keepdims=True) + NORM_EPS) * gain

    span = 2 * rows

    def block(n, places):
        for m, yy in enumerate(places):
            for i in range(2):
                xn[(2 * m + i) * rows : (2 * m + i + 1) * rows, :] = modulate(lat[yy * 2 + i], 0)
        spots = [pl.ds(pl.multiple_of(yy * span, span), span) for yy in places]
        turns = [(cos_ref[:, :, at], sin_ref[:, :, at]) for at in spots]
        key = unit(jnp.dot(xn[...], wk[...], preferred_element_type=F32), kgain)
        val = jnp.dot(xn[...], wv[...], preferred_element_type=F32)
        for m in range(2):
            at = slice((2 * n + m) * span, (2 * n + m + 1) * span)
            kb[z, at, :] = turn(key[m * span : (m + 1) * span].T, *turns[m]).T.astype(BF16)
        vb[z, n] = val.T.astype(BF16)
        for way, dz in ((0, 1), (1, z_count - 1)):
            peer = ((z + dz) % z_count) * x_count + x
            for one in kv_copy(kb, vb, kv_send, kv_recv, z, n, way, peer, t):
                go(one)
        full = jnp.dot(xn[...], wq[...], preferred_element_type=F32)
        for m in range(2):
            for h in range(full.shape[1] // head_dim):
                yh = unit(full[m * span : (m + 1) * span, h * head_dim : (h + 1) * head_dim], qgain)
                qb[x, h, :, spots[m]] = turn(yh.T, *turns[m]).astype(BF16)
            for d in (1, x_count - 1):
                peer = z * x_count + (x + d) % x_count
                go(q_copy(qb, q_send, q_recv, x, places[m], 2 * n + m, d, peer, t))

    def pair_wait(yy):
        other = yy * 2 + 1 - c
        remote(lat.at[other], lat.at[other], pair_send.at[0], pair_recv.at[other], (s, t)).wait_recv()

    spots_y = [(y + step) % y_count for step in (0, 1, y_count - 1, 2)]
    with jax.named_scope("far"):
        lat_half(far, 0, 0, t).wait_recv()
        lat_half(far, 1, 0, t).wait_recv()
        go(pair(far, 3))
        pair_wait(spots_y[0])
        pair_wait(spots_y[1])
    with jax.named_scope("block"):
        block(0, spots_y[:2])
    cn = modulate(ctx[...], 1)
    kc = jnp.dot(cn, wk[...], preferred_element_type=F32)
    vc = jnp.dot(cn, wv[...], preferred_element_type=F32)
    cb[z, 0] = unit(kc, kgain).astype(BF16)
    cb[z, 1] = vc.astype(BF16)
    for j in range(1, z_count):
        go(remote(cb.at[z], cb.at[z], c_send.at[j], c_recv.at[z], (((z + j) % z_count) * x_count + x, t)))
    with jax.named_scope("far"):
        pair_wait(spots_y[2])
        pair_wait(spots_y[3])
    with jax.named_scope("block"):
        block(1, spots_y[2:])
    for j, yy in enumerate(spots_y):
        go(q_copy(qb, q_send, q_recv, x, yy, j, 2, z * x_count + (x + 2) % x_count, t))
    return started


def wo_half(wo, wo_send, wo_recv, src, n, send, s, dev):
    half = wo.shape[1] // 2
    ref = wo.at[src, pl.ds(n * half, half)]
    return remote(ref, ref, wo_send.at[send], wo_recv.at[src, n], (s, dev))


def wo_pair(wo, send_sem, recv_sem, src, send, s, dev):
    return remote(wo.at[src], wo.at[src], send_sem.at[send], recv_sem.at[src], (s, dev))


def kv_copy(kb, vb, kv_send, kv_recv, src, n, way, peer, t, which=(0, 1)):
    half = kb.shape[1] // 2
    both = [
        remote(
            kb.at[src, pl.ds(n * half, half)], kb.at[src, pl.ds(n * half, half)],
            kv_send.at[0, src, way, n], kv_recv.at[0, src, n], (peer, t),
        ),
        remote(
            vb.at[src, n], vb.at[src, n], kv_send.at[1, src, way, n], kv_recv.at[1, src, n], (peer, t)
        ),
    ]
    return [both[i] for i in which]


def q_copy(qb, q_send, q_recv, owner, yy, j, d, peer, t):
    span = qb.shape[3] // 4
    at = pl.ds(pl.multiple_of(yy * span, span), span)
    ref = qb.at[owner, :, :, at]
    return remote(ref, ref, q_send.at[d, j], q_recv.at[owner, yy], (peer, t))


def attend_kernel(
    sp_count, x_count, lift,
    tp_count, qb, kb, vb, cb, q_send, q_recv, kv_send, kv_recv, c_send, c_recv,
    wo, wo_send, wo_recv, wo_pair_send, wo_pair_recv,
    att, top, tot, acc, ob, ib, om, im, o_send, o_recv, m_send, m_recv, started,
):
    s, t = lax.axis_index("sp"), lax.axis_index("tp")
    z, x = s // x_count, s % x_count
    z_count = sp_count // x_count
    heads, head_dim, rows = qb.shape[1:]
    factor = head_dim ** (-0.5) * math.log2(math.e)
    bias = lift * head_dim**0.5

    top[...] = jnp.full_like(top, -1e30)
    tot[...] = jnp.zeros_like(tot)
    acc[...] = jnp.zeros_like(acc)

    y, c = t // 2, t % 2
    y_count = tp_count // 2
    partner = y * 2 + 1 - c
    right, left, over = [((y + j) % y_count) * 2 + c for j in (1, y_count - 1, 2)]

    def wo_arrive(src, n):
        wo_half(wo, wo_send, wo_recv, src, n, 0, s, t).wait_recv()

    def go(one):
        one.start()
        started.append(one)

    def at_z(k):
        return (z + k + z_count) % z_count

    def soft(d, h, sc, values):
        i = d * heads + h
        old = top[i]
        new = jnp.maximum(old, jnp.max(sc, axis=0, keepdims=True))
        p = jnp.exp2((sc - new) * factor)
        f = jnp.exp2((old - new) * factor)
        top[i] = new
        tot[i] = tot[i] * f + jnp.sum(p, axis=0, keepdims=True)
        p = p.astype(BF16)
        new_acc = acc[i] * f
        step = p.shape[0] // len(values)
        for n, one in enumerate(values):
            new_acc = new_acc + jnp.dot(one, p[n * step : (n + 1) * step], preferred_element_type=F32)
        acc[i] = new_acc

    def units(pairs, with_ctx=None):
        todo = []
        for kv, d in pairs:
            for h in range(heads):
                todo.append((kv, d, h))

        def scores(one):
            kv, d, h = one
            return jnp.dot(kb[kv], qb[(x + d) % x_count, h], preferred_element_type=F32)

        ahead = [scores(one) for one in todo[:2]]
        for n, one in enumerate(todo):
            sc = ahead.pop(0)
            if n + 2 < len(todo):
                ahead.append(scores(todo[n + 2]))
            kv, d, h = one
            soft(d, h, sc, [vb[kv, 0], vb[kv, 1]])

    def forward(k, n, which_r=(0, 1), which_l=(0, 1)):
        for sign, way, which in ((-1, 0, which_r), (1, 1, which_l)):
            src = at_z(sign * k)
            for one in kv_copy(kb, vb, kv_send, kv_recv, src, n, 0, s, t):
                one.wait_recv()
            peer = at_z(1 if way == 0 else -1) * x_count + x
            for one in kv_copy(kb, vb, kv_send, kv_recv, src, n, way, peer, t, which):
                go(one)

    def q_arrive(d):
        owner = (x + d) % x_count
        for yy in range(4):
            q_copy(qb, q_send, q_recv, owner, yy, 0, 0, s, t).wait_recv()

    def both(k, d):
        return [(at_z(-k), d), (at_z(k), d)]

    with jax.named_scope("own"):
        units([(z, 0)])
    with jax.named_scope("forward1"):
        forward(1, 0)
        forward(1, 1)
    with jax.named_scope("q1"):
        q_arrive(3)
        q_arrive(1)
    with jax.named_scope("units1"):
        units([(z, 3), (z, 1)] + both(1, 3))
    with jax.named_scope("forward2"):
        forward(2, 0)
    with jax.named_scope("units2"):
        units(both(1, 1))
    with jax.named_scope("forward2"):
        forward(2, 1)
    with jax.named_scope("wo1"):
        wo_arrive(left, 0)
        go(wo_half(wo, wo_send, wo_recv, left, 0, 4, s, right))
        wo_arrive(right, 1)
        go(wo_half(wo, wo_send, wo_recv, right, 1, 5, s, left))
    with jax.named_scope("q2"):
        q_arrive(2)
    with jax.named_scope("units3"):
        units([(z, 2)] + both(1, 2) + both(2, 2))
    with jax.named_scope("forward3"):
        forward(3, 0, (0,), (1,))
    with jax.named_scope("units4"):
        units(both(2, 3))
    with jax.named_scope("forward3"):
        forward(3, 1, (0,), (1,))
    with jax.named_scope("units5"):
        units(both(2, 1) + both(3, 2))
    for j in range(1, z_count):
        src = at_z(j)
        remote(cb.at[src], cb.at[src], c_send.at[0], c_recv.at[src], (s, t)).wait_recv()
    ckeys = jnp.concatenate([cb[j, 0] for j in range(z_count)], axis=0)
    cvals = jnp.concatenate([cb[j, 1] for j in range(z_count)], axis=0).astype(F32).T.astype(BF16)

    def context(d):
        for h in range(heads):
            sc = jnp.dot(ckeys, qb[(x + d) % x_count, h], preferred_element_type=F32) + bias
            soft(d, h, sc, [cvals])

    def gift(d):
        peer = z * x_count + (x + d) % x_count
        return [
            remote(a.at[d - 1], b.at[d - 1], u.at[d - 1], v.at[d - 1], (peer, t))
            for a, b, u, v in ((om, im, m_send, m_recv), (ob, ib, o_send, o_recv))
        ]

    def give(d):
        for h in range(heads):
            i = d * heads + h
            ob[d - 1, h] = (acc[i] / tot[i]).astype(BF16)
            om[d - 1, h, 0:1, :] = top[i]
            om[d - 1, h, 1:2, :] = tot[i]
        for one in gift(d):
            one.start()

    with jax.named_scope("forward4"):
        for n in range(2):
            for one in kv_copy(kb, vb, kv_send, kv_recv, at_z(4), n, 0, s, t):
                one.wait_recv()
    with jax.named_scope("give2"):
        units([(at_z(4), 2)])
        context(2)
        give(2)
    with jax.named_scope("wo2"):
        wo_arrive(left, 1)
        go(wo_pair(wo, wo_pair_send, wo_pair_recv, left, 1, s, partner))
        wo_arrive(right, 0)
        go(wo_pair(wo, wo_pair_send, wo_pair_recv, right, 2, s, partner))

    def beside(i, carry):
        d = 3 - 2 * i
        units(both(3, d) + [(at_z(4), d)])
        context(d)
        give(d)
        return carry

    with jax.named_scope("give31"):
        lax.fori_loop(0, 2, beside, 0)

    def last(k, carry):
        units(both(k, 0))
        return carry

    with jax.named_scope("last"):
        lax.fori_loop(1, 4, last, 0)
        units([(at_z(4), 0)])
        context(0)
    with jax.named_scope("wo3"):
        for n in range(2):
            wo_arrive(over, n)
        go(wo_pair(wo, wo_pair_send, wo_pair_recv, over, 3, s, partner))
    with jax.named_scope("drain"):
        for one in started[:-1]:
            one.wait_send()
        del started[:-1]
    for d in (2, 3, 1):
        started.extend(gift(d))
    with jax.named_scope("owait"):
        for d in range(1, x_count):
            for a, b, u, v in ((om, im, m_send, m_recv), (ob, ib, o_send, o_recv)):
                remote(a.at[d - 1], b.at[d - 1], u.at[d - 1], v.at[d - 1], (s, t)).wait_recv()
    with jax.named_scope("merge"):
        for h in range(heads):
            best = top[h]
            for d in range(1, x_count):
                best = jnp.maximum(best, im[d - 1, h, 0:1, :])
            f = jnp.exp2((top[h] - best) * factor)
            value, weight = acc[h] * f, tot[h] * f
            for d in range(1, x_count):
                w = im[d - 1, h, 1:2, :] * jnp.exp2(
                    (im[d - 1, h, 0:1, :] - best) * factor
                )
                value = value + ib[d - 1, h].astype(F32) * w
                weight = weight + w
            att[:, h * head_dim : (h + 1) * head_dim] = (value / weight).T.astype(BF16)


def mix_kernel(
    tp_count, att, wo, wo_pair_send, wo_pair_recv, lat, gate_ref, out_ref, mixed, af, a_send, a_recv, started
):
    s, t = lax.axis_index("sp"), lax.axis_index("tp")
    y, c = t // 2, t % 2
    y_count = tp_count // 2
    partner = y * 2 + 1 - c
    rows, width = mixed.shape

    def slab(dev):
        return pl.ds(pl.multiple_of(dev * rows, rows), rows)

    order = [((y + j) % y_count) * 2 + k for j in (1, y_count - 1, 2) for k in (c, 1 - c)]
    for n, dev in enumerate([partner] + order[4:] + order[:4]):
        one = remote(att.at[slab(dev)], af.at[t], a_send.at[n], a_recv.at[t], (s, dev))
        one.start()
        started.append(one)
    mixed[...] = jnp.dot(att[slab(t), :], wo[t], preferred_element_type=F32)
    for n, dev in enumerate([partner] + order):
        remote(att.at[slab(dev)], af.at[dev], a_send.at[0], a_recv.at[dev], (s, t)).wait_recv()
        if n % 2 == 0:
            wo_pair(wo, wo_pair_send, wo_pair_recv, dev, 0, s, t).wait_recv()
        mixed[...] = mixed[...] + jnp.dot(af[dev], wo[dev], preferred_element_type=F32)
    value = mixed[...]
    inv = lax.rsqrt(jnp.mean(value * value, axis=-1, keepdims=True) + NORM_EPS)
    out_ref[...] = (lat[t].astype(F32) + gate_ref[...] * (value * inv)).astype(BF16)


def whole_kernel(sp_count, tp_count, x_count, head_dim, lift, counts, *refs):
    (
        cond, cond_1, mw, lat, ctx, wq, wk, wv, qg, kg, freq, wo_hbm,
        out, qb, kb, vb, cb, gate, att, wo, wo_sem, *rest,
    ) = refs
    groups, start = [], 0
    for count in counts:
        groups.append(rest[start : start + count])
        start += count
    links, wo_sems, front_scratch, middle_scratch, last_scratch = groups
    lat_all = front_scratch[1]
    started = front_kernel(
        sp_count, tp_count, x_count, head_dim, cond, cond_1, mw, lat, ctx, wq, wk, wv, qg, kg, freq,
        qb, kb, vb, cb, gate, *links, *front_scratch, wo_hbm, wo, wo_sem, *wo_sems,
    )
    with jax.named_scope("attn"):
        attend_kernel(
            sp_count, x_count, lift, tp_count, qb, kb, vb, cb, *links, wo, *wo_sems,
            att, *middle_scratch, started,
        )
    with jax.named_scope("mix"):
        mix_kernel(tp_count, att, wo, *wo_sems[2:], lat_all, gate, out, *last_scratch, started)
    for one in started:
        one.wait_send()


ANY = pl.BlockSpec(memory_space=pl.ANY)
VM = pl.BlockSpec(memory_space=pltpu.VMEM)
DMA = pltpu.SemaphoreType.DMA


def body(
    latents,
    context,
    cond,
    ctx_cond,
    mod_weight,
    query_weight,
    key_matrix,
    value_matrix,
    out_weight,
    query_gain,
    key_gain,
):
    sp_count, tp_count = lax.axis_size("sp"), lax.axis_size("tp")
    x_count = row_size(sp_count)
    rows, width = latents.shape
    ctx_rows = context.shape[0]
    head_dim = query_gain.shape[0]
    heads = query_weight.shape[1] // head_dim
    all_rows = rows * tp_count
    mod_cols = mod_weight.shape[1]
    quarter = head_dim // 4
    freq = np.float32(ROPE_BASE) ** (-np.arange(quarter, dtype=np.float32) / np.float32(quarter))
    freq = jnp.asarray(freq[:, None], F32)
    lift = math.log(sp_count * all_rows / (2.0 * sp_count * ctx_rows))
    y_count = tp_count // 2
    far = max(y_count - 1, 1)
    z_count = sp_count // x_count
    shared = [
        pltpu.VMEM((x_count, heads, head_dim, all_rows), BF16),
        pltpu.VMEM((z_count, all_rows, head_dim), BF16),
        pltpu.VMEM((z_count, 2, head_dim, all_rows // 2), BF16),
        pltpu.VMEM((z_count, 2, ctx_rows, head_dim), BF16),
        pltpu.VMEM((1, width), F32),
        pltpu.VMEM((all_rows, heads * head_dim), BF16),
        pltpu.VMEM((tp_count, *out_weight.shape), BF16),
        DMA((1,)),
    ]
    wo_sems = [DMA((6,)), DMA((tp_count, 2)), DMA((4,)), DMA((tp_count,))]
    links = [
        DMA((x_count, y_count)),
        DMA((x_count, y_count)),
        DMA((2, z_count, 2, 2)),
        DMA((2, z_count, 2)),
        DMA((z_count,)),
        DMA((z_count,)),
    ]
    front = [
        pltpu.VMEM(mod_weight.shape, F32),
        pltpu.VMEM((tp_count, rows, width), BF16),
        pltpu.VMEM(query_weight.shape, BF16),
        pltpu.VMEM(key_matrix.shape, BF16),
        pltpu.VMEM(value_matrix.shape, BF16),
        pltpu.VMEM((sp_count, 2, mod_cols), F32),
        pltpu.VMEM((tp_count, 2, mod_cols), F32),
        pltpu.VMEM((2, mod_cols * tp_count), F32),
        pltpu.VMEM((4 * rows, width), BF16),
        pltpu.VMEM((ctx_rows, width), BF16),
        pltpu.VMEM((2, quarter, all_rows), F32),
        pltpu.VMEM((2, quarter, all_rows), F32),
        pltpu.VMEM((1, cond.shape[0]), F32),
        pltpu.VMEM((1, cond.shape[0]), F32),
        pltpu.VMEM((1, head_dim), F32),
        pltpu.VMEM((1, head_dim), F32),
        pltpu.VMEM((quarter, 1), F32),
        DMA((11,)),
        DMA((6,)),
        DMA((tp_count, 2)),
        DMA((4,)),
        DMA((tp_count,)),
        DMA((sp_count,)),
        DMA((sp_count,)),
        DMA((tp_count,)),
        DMA((tp_count,)),
    ]
    far = x_count - 1
    middle = [
        pltpu.VMEM((x_count * heads, 1, all_rows), F32),
        pltpu.VMEM((x_count * heads, 1, all_rows), F32),
        pltpu.VMEM((x_count * heads, head_dim, all_rows), F32),
        pltpu.VMEM((far, heads, head_dim, all_rows), BF16),
        pltpu.VMEM((far, heads, head_dim, all_rows), BF16),
        pltpu.VMEM((far, heads, 2, all_rows), F32),
        pltpu.VMEM((far, heads, 2, all_rows), F32),
        DMA((far,)),
        DMA((far,)),
        DMA((far,)),
        DMA((far,)),
    ]
    last = [
        pltpu.VMEM((rows, width), F32),
        pltpu.VMEM((tp_count, rows, heads * head_dim), BF16),
        DMA((tp_count,)),
        DMA((tp_count,)),
    ]
    groups = (links, wo_sems, front, middle, last)
    counts = tuple(len(one) for one in groups)
    return pl.pallas_call(
        functools.partial(
            whole_kernel, sp_count, tp_count, x_count, head_dim, lift, counts
        ),
        out_shape=jax.ShapeDtypeStruct((rows, width), BF16),
        in_specs=[ANY] * 12,
        out_specs=VM,
        scratch_shapes=shared + sum(groups, []),
        compiler_params=pltpu.CompilerParams(
            collective_id=0, has_side_effects=True, vmem_limit_bytes=VMEM_BYTES,
        ),
        name="whole",
    )(
        cond[None], ctx_cond[None], mod_weight, latents, context, query_weight, key_matrix, value_matrix,
        query_gain[None], key_gain[None], freq, out_weight,
    )


def solution(mesh):
    placed = (
        P(("sp", "tp"), None),
        P("sp", None),
        P("sp"),
        P("sp"),
        P("sp", "tp"),
        P(None, "tp"),
        P(None, "tp"),
        P(None, "tp"),
        P("tp", None),
        P(),
        P(),
    )
    return jax.shard_map(
        body, mesh=mesh, in_specs=placed, out_specs=P(("sp", "tp"), None), check_vma=False
    )
```

```python
import functools
import math

import jax
import jax.numpy as jnp
import numpy as np
from jax import lax
from jax.experimental import pallas as pl
from jax.experimental.pallas import tpu as pltpu
from jax.sharding import PartitionSpec as P

GRID_W = 64
NORM_EPS = 1e-06
ROPE_BASE = 10000.0
MESH = pl.DeviceIdType.MESH
BF16 = jnp.bfloat16
F32 = jnp.float32
VMEM_BYTES = 67043328


def row_size(sp_count):
    size = 1
    while 4 * size * size <= sp_count:
        size *= 2
    return size


def remote(src, dst, send, recv, dev):
    return pltpu.make_async_remote_copy(
        src_ref=src, dst_ref=dst, send_sem=send, recv_sem=recv, device_id=dev, device_id_type=MESH
    )


def front_kernel(
    sp_count, tp_count, x_count, head_dim,
    cond_hbm, cond_1_hbm, mw_hbm, lat_hbm, ctx_hbm, wq_hbm, wk_hbm, wv_hbm, qg_hbm, kg_hbm, freq_hbm,
    qb, kb, vb, cb, gate_ref, q_send, q_recv, kv_send, kv_recv, c_send, c_recv,
    mw, lat, wq, wk, wv, part, tot, mod, xn, ctx, cos_ref, sin_ref,
    cond_ref, cond_1_ref, qg_ref, kg_ref, freq_ref, load_sem,
    lat_send, lat_recv, pair_send, pair_recv, part_send, part_recv, tot_send, tot_recv,
    wo_hbm, wo, wo_sem, wo_send, wo_recv, wo_pair_send, wo_pair_recv,
):
    s, t = lax.axis_index("sp"), lax.axis_index("tp")
    y, c = t // 2, t % 2
    z, x = s // x_count, s % x_count
    z_count = sp_count // x_count
    y_count = tp_count // 2
    partner = y * 2 + 1 - c
    rows = lat.shape[1]
    half = rows // 2
    width = lat.shape[2]
    model_cols = mod.shape[1]
    right, left, far = [((y + j) % y_count) * 2 + c for j in (1, y_count - 1, 2)]

    loads = [
        pltpu.make_async_copy(a, b, load_sem.at[i])
        for i, (a, b) in enumerate(
            (
                (cond_hbm, cond_ref), (cond_1_hbm, cond_1_ref), (mw_hbm, mw), (lat_hbm, lat.at[t]),
                (freq_hbm, freq_ref), (kg_hbm, kg_ref), (qg_hbm, qg_ref), (ctx_hbm, ctx),
                (wk_hbm, wk), (wv_hbm, wv), (wq_hbm, wq),
            )
        )
    ]
    for one in loads[:4]:
        one.start()

    barrier = pltpu.get_barrier_semaphore()
    for j in range(1, sp_count):
        pl.semaphore_signal(barrier, inc=1, device_id=((s + j) % sp_count, t), device_id_type=MESH)
    for j in range(1, tp_count):
        pl.semaphore_signal(barrier, inc=1, device_id=(s, (t + j) % tp_count), device_id_type=MESH)

    for one in loads[4:]:
        one.start()
    wo_load = pltpu.make_async_copy(wo_hbm, wo.at[t], wo_sem.at[0])
    wo_load.start()
    for one in loads[:3]:
        one.wait()
    lines = lax.broadcasted_iota(jnp.int32, (8, cond_ref.shape[1]), 0)
    cond = jnp.where(lines == 0, cond_ref[...], jnp.where(lines == 1, cond_1_ref[...], 0.0))
    cond = cond * jax.nn.sigmoid(cond)
    part[s] = jnp.dot(
        cond, mw[...], precision=lax.Precision.HIGHEST, preferred_element_type=F32
    )[:2]
    loads[3].wait()
    with jax.named_scope("barrier"):
        pl.semaphore_wait(barrier, sp_count + tp_count - 2)

    started = []

    def go(one):
        one.start()
        started.append(one)

    def lat_half(src, n, send, dev):
        at = pl.ds(n * half, half)
        return remote(
            lat.at[src, at], lat.at[src, at], lat_send.at[send], lat_recv.at[src // 2, n], (s, dev)
        )

    def pair(src, send):
        return remote(lat.at[src], lat.at[src], pair_send.at[send], pair_recv.at[src // 2], (s, partner))

    for j in range(1, sp_count):
        remote(part.at[s], part.at[s], part_send.at[0], part_recv.at[0], ((s + j) % sp_count, t)).start()
    others = part.at[pl.ds(0, sp_count - 1)]
    sent_part = remote(others, others, part_send.at[0], part_recv.at[0], (s, t))
    started.append(sent_part)
    go(lat_half(t, 0, 0, right))
    go(lat_half(t, 1, 1, left))
    go(lat_half(t, 1, 2, right))
    go(lat_half(t, 0, 3, left))
    go(pair(t, 0))

    loads[4].wait()
    where = s * cos_ref.shape[2] + lax.broadcasted_iota(jnp.int32, cos_ref.shape[1:], 1)
    for n, place in enumerate((where // GRID_W, where % GRID_W)):
        angle = place.astype(F32) * freq_ref[...]
        cos_ref[n] = jnp.cos(angle)
        sin_ref[n] = jnp.sin(angle)

    with jax.named_scope("modsum"):
        sent_part.wait_recv()
        total = part[0]
        for j in range(1, sp_count):
            total = total + part[j]
        tot[t] = total
    for j in range(1, tp_count):
        remote(tot.at[t], tot.at[t], tot_send.at[0], tot_recv.at[0], (s, (t + j) % tp_count)).start()

    others = tot.at[pl.ds(0, tp_count - 1)]
    sent_tot = remote(others, others, tot_send.at[0], tot_recv.at[0], (s, t))
    started.append(sent_tot)

    with jax.named_scope("latwait"):
        lat_half(left, 0, 0, t).wait_recv()
        go(lat_half(left, 0, 4, right))
        lat_half(right, 1, 0, t).wait_recv()
        go(lat_half(right, 1, 5, left))
        lat_half(left, 1, 0, t).wait_recv()
        go(pair(left, 1))
        lat_half(right, 0, 0, t).wait_recv()
        go(pair(right, 2))

    wo_load.wait()
    for src, n, send, dev in ((t, 0, 0, right), (t, 1, 1, left), (t, 1, 2, right), (t, 0, 3, left)):
        go(wo_half(wo, wo_send, wo_recv, src, n, send, s, dev))
    go(wo_pair(wo, wo_pair_send, wo_pair_recv, t, 0, s, partner))

    with jax.named_scope("totwait"):
        sent_tot.wait_recv()
    cols = model_cols // tp_count
    for j in range(tp_count):
        mod[:, j * cols : (j + 1) * cols] = tot[j]
    gate_ref[...] = mod[0:1, 2 * width :]

    def modulate(x_rows, r):
        x_rows = x_rows.astype(F32)
        scaled = x_rows * lax.rsqrt(jnp.mean(x_rows * x_rows, axis=-1, keepdims=True) + NORM_EPS)
        shift, scale = mod[r : r + 1, :width], mod[r : r + 1, width : 2 * width]
        return (scaled * (1.0 + scale) + shift).astype(BF16)

    with jax.named_scope("loadwait"):
        for one in loads[5:]:
            one.wait()

    q4 = head_dim // 4
    qgain, kgain = qg_ref[...], kg_ref[...]

    def turn(yt, cos, sin):
        out = []
        for n in range(2):
            a = yt[2 * n * q4 : (2 * n + 1) * q4]
            b = yt[(2 * n + 1) * q4 : (2 * n + 2) * q4]
            out += [a * cos[n] - b * sin[n], b * cos[n] + a * sin[n]]
        return jnp.concatenate(out, axis=0)

    def unit(yh, gain):
        return yh * lax.rsqrt(jnp.mean(yh * yh, axis=-1, keepdims=True) + NORM_EPS) * gain

    span = 2 * rows

    def block(n, places):
        for m, yy in enumerate(places):
            for i in range(2):
                xn[(2 * m + i) * rows : (2 * m + i + 1) * rows, :] = modulate(lat[yy * 2 + i], 0)
        spots = [pl.ds(pl.multiple_of(yy * span, span), span) for yy in places]
        turns = [(cos_ref[:, :, at], sin_ref[:, :, at]) for at in spots]
        key = unit(jnp.dot(xn[...], wk[...], preferred_element_type=F32), kgain)
        val = jnp.dot(xn[...], wv[...], preferred_element_type=F32)
        for m in range(2):
            at = slice((2 * n + m) * span, (2 * n + m + 1) * span)
            kb[z, at, :] = turn(key[m * span : (m + 1) * span].T, *turns[m]).T.astype(BF16)
        vb[z, n] = val.T.astype(BF16)
        for way, dz in ((0, 1), (1, z_count - 1)):
            peer = ((z + dz) % z_count) * x_count + x
            copies, all_sent = kv_copy(kb, vb, kv_send, kv_recv, z, n, 0, way, peer, t)
            for one in copies:
                one.start()
            started.append(all_sent)
        full = jnp.dot(xn[...], wq[...], preferred_element_type=F32)
        for m in range(2):
            for h in range(full.shape[1] // head_dim):
                yh = unit(full[m * span : (m + 1) * span, h * head_dim : (h + 1) * head_dim], qgain)
                qb[x, h, :, spots[m]] = turn(yh.T, *turns[m]).astype(BF16)
            for d in (1, x_count - 1):
                peer = z * x_count + (x + d) % x_count
                q_copy(qb, q_send, q_recv, x, places[m], d, peer, t).start()

    def pair_wait(yy):
        other = yy * 2 + 1 - c
        remote(lat.at[other], lat.at[other], pair_send.at[0], pair_recv.at[yy], (s, t)).wait_recv()

    def context_rows():
        cn = modulate(ctx[...], 1)
        kc = jnp.dot(cn, wk[...], preferred_element_type=F32)
        vc = jnp.dot(cn, wv[...], preferred_element_type=F32)
        cb[z, 0] = unit(kc, kgain).astype(BF16)
        cb[z, 1] = vc.astype(BF16)
        for j in range(1, z_count):
            remote(
                cb.at[z], cb.at[z], c_send.at[0], c_recv.at[0], (((z + j) % z_count) * x_count + x, t)
            ).start()
        others = cb.at[pl.ds(0, z_count - 1)]
        started.append(remote(others, others, c_send.at[0], c_recv.at[0], (s, t)))

    spots_y = [(y + step) % y_count for step in (0, 1, y_count - 1, 2)]
    with jax.named_scope("far"):
        lat_half(far, 0, 0, t).wait_recv()
        lat_half(far, 1, 0, t).wait_recv()
        go(pair(far, 3))
        pair_wait(spots_y[0])
        pair_wait(spots_y[1])
    with jax.named_scope("block"):
        block(0, spots_y[:2])
    with jax.named_scope("far"):
        pair_wait(spots_y[2])
        pair_wait(spots_y[3])
    with jax.named_scope("block"):
        block(1, spots_y[2:])
    for yy in spots_y:
        q_copy(qb, q_send, q_recv, x, yy, 2, z * x_count + (x + 2) % x_count, t).start()
    for d in range(1, x_count):
        started.append(remote(qb.at[x], qb.at[x], q_send.at[d], q_recv.at[x], (s, t)))
    return started, context_rows


def wo_half(wo, wo_send, wo_recv, src, n, send, s, dev):
    half = wo.shape[1] // 2
    ref = wo.at[src, pl.ds(n * half, half)]
    return remote(ref, ref, wo_send.at[send], wo_recv.at[src // 2, n], (s, dev))


def wo_pair(wo, send_sem, recv_sem, src, send, s, dev):
    return remote(wo.at[src], wo.at[src], send_sem.at[send], recv_sem.at[src // 2], (s, dev))


def kv_copy(kb, vb, kv_send, kv_recv, src, n, hop, way, peer, t, which=(0, 1)):
    half = kb.shape[1] // 2
    key = kb.at[src, pl.ds(n * half, half)]
    refs = [(key, vb.at[src, n])[i] for i in which]
    both = [
        remote(ref, ref, kv_send.at[hop, way, n], kv_recv.at[src, n], (peer, t)) for ref in refs
    ]
    whole = kb.at[src] if len(which) == 2 else key
    return both, remote(whole, whole, kv_send.at[hop, way, n], kv_recv.at[src, n], (peer, t))


def q_copy(qb, q_send, q_recv, owner, yy, d, peer, t):
    span = qb.shape[3] // 4
    at = pl.ds(pl.multiple_of(yy * span, span), span)
    ref = qb.at[owner, :, :, at]
    return remote(ref, ref, q_send.at[d], q_recv.at[owner], (peer, t))


def attend_kernel(
    sp_count, x_count, lift,
    tp_count, qb, kb, vb, cb, q_send, q_recv, kv_send, kv_recv, c_send, c_recv,
    wo, wo_send, wo_recv, wo_pair_send, wo_pair_recv,
    att, top, tot, acc, ob, ib, om, im, o_send, o_recv, m_send, m_recv, started, context_rows,
):
    s, t = lax.axis_index("sp"), lax.axis_index("tp")
    z, x = s // x_count, s % x_count
    z_count = sp_count // x_count
    heads, head_dim, rows = qb.shape[1:]
    factor = head_dim ** (-0.5) * math.log2(math.e)
    bias = lift * head_dim**0.5

    top[...] = jnp.full_like(top, -1e30)
    tot[...] = jnp.zeros_like(tot)
    acc[...] = jnp.zeros_like(acc)

    y, c = t // 2, t % 2
    y_count = tp_count // 2
    partner = y * 2 + 1 - c
    right, left, over = [((y + j) % y_count) * 2 + c for j in (1, y_count - 1, 2)]

    def wo_arrive(src, n):
        wo_half(wo, wo_send, wo_recv, src, n, 0, s, t).wait_recv()

    def go(one):
        one.start()
        started.append(one)

    def at_z(k):
        return (z + k + z_count) % z_count

    def soft(d, h, sc, values):
        i = d * heads + h
        old = top[i]
        new = jnp.maximum(old, jnp.max(sc, axis=0, keepdims=True))
        p = jnp.exp2((sc - new) * factor)
        f = jnp.exp2((old - new) * factor)
        top[i] = new
        tot[i] = tot[i] * f + jnp.sum(p, axis=0, keepdims=True)
        p = p.astype(BF16)
        new_acc = acc[i] * f
        step = p.shape[0] // len(values)
        for n, one in enumerate(values):
            new_acc = new_acc + jnp.dot(one, p[n * step : (n + 1) * step], preferred_element_type=F32)
        acc[i] = new_acc

    def entries(pairs, hs=(0, 1), context=None):
        todo = [(kv, d, h) for kv, d in pairs for h in hs]
        return todo + ([] if context is None else [(None, context, h) for h in hs])

    def units(pairs, context=None):
        work(entries(pairs, context=context))

    def work(todo, then={}):
        if any(one[0] is None for one in todo):
            ckeys = jnp.concatenate([cb[j, 0] for j in range(z_count)], axis=0)
            cvals = jnp.concatenate([cb[j, 1] for j in range(z_count)], axis=0)
            cvals = cvals.astype(F32).T.astype(BF16)

        def scores(one):
            kv, d, h = one
            query = qb[(x + d) % x_count, h]
            if kv is None:
                return jnp.dot(ckeys, query, preferred_element_type=F32) + bias
            return jnp.dot(kb[kv], query, preferred_element_type=F32)

        ahead = [scores(one) for one in todo[:2]]
        for n, one in enumerate(todo):
            sc = ahead.pop(0)
            if n + 2 < len(todo):
                ahead.append(scores(todo[n + 2]))
            kv, d, h = one
            soft(d, h, sc, [cvals] if kv is None else [vb[kv, 0], vb[kv, 1]])
            if n in then:
                then[n]()

    def kv_wait(src, n):
        kv_copy(kb, vb, kv_send, kv_recv, src, n, 0, 0, s, t)[1].wait_recv()

    def forward(k, n, which_r=(0, 1), which_l=(0, 1)):
        for sign, way, which in ((-1, 0, which_r), (1, 1, which_l)):
            src = at_z(sign * k)
            kv_wait(src, n)
            peer = at_z(1 if way == 0 else -1) * x_count + x
            copies, all_sent = kv_copy(kb, vb, kv_send, kv_recv, src, n, k, way, peer, t, which)
            for one in copies:
                one.start()
            started.append(all_sent)

    def q_arrive(d):
        owner = (x + d) % x_count
        remote(qb.at[owner], qb.at[owner], q_send.at[0], q_recv.at[owner], (s, t)).wait_recv()

    def both(k, d):
        return [(at_z(-k), d), (at_z(k), d)]

    with jax.named_scope("own"):
        units([(z, 0)])
    with jax.named_scope("context"):
        context_rows()
    with jax.named_scope("forward1"):
        forward(1, 0)
        forward(1, 1)
    with jax.named_scope("q1"):
        q_arrive(3)
        q_arrive(1)
    with jax.named_scope("units1"):
        units([(z, 3), (z, 1)] + both(1, 3))
    with jax.named_scope("forward2"):
        forward(2, 0)
    with jax.named_scope("units2"):
        units(both(1, 1))
    with jax.named_scope("forward2"):
        forward(2, 1)
    with jax.named_scope("wo1"):
        wo_arrive(left, 0)
        go(wo_half(wo, wo_send, wo_recv, left, 0, 4, s, right))
        wo_arrive(right, 1)
        go(wo_half(wo, wo_send, wo_recv, right, 1, 5, s, left))
    with jax.named_scope("q2"):
        q_arrive(2)
    with jax.named_scope("units3"):
        units([(z, 2)] + both(1, 2))
    with jax.named_scope("forward3"):
        forward(3, 0, (0,), (1,))
    with jax.named_scope("units4"):
        units(both(2, 2))
    with jax.named_scope("forward3"):
        forward(3, 1, (0,), (1,))
    with jax.named_scope("units5"):
        units(both(2, 3) + both(2, 1) + both(3, 2))
    others = cb.at[pl.ds(0, z_count - 1)]
    remote(others, others, c_send.at[0], c_recv.at[0], (s, t)).wait_recv()

    def gift(i, h, d):
        peer = z * x_count + (x + d) % x_count
        return [
            remote(a.at[i, h], b.at[i, h], u.at[i, h], v.at[i, h], (peer, t))
            for a, b, u, v in ((om, im, m_send, m_recv), (ob, ib, o_send, o_recv))
        ]

    def merged(i, h, parts):
        best = top[i * heads + h]
        for part in parts:
            best = jnp.maximum(best, im[part, h, 0:1, :])
        f = jnp.exp2((top[i * heads + h] - best) * factor)
        value, weight = acc[i * heads + h] * f, tot[i * heads + h] * f
        for part in parts:
            w = im[part, h, 1:2, :] * jnp.exp2((im[part, h, 0:1, :] - best) * factor)
            value = value + ib[part, h].astype(F32) * w
            weight = weight + w
        return value / weight, best, weight

    def give(i, h, d, to, parts=()):
        value, best, weight = merged(d, h, parts)
        ob[i, h] = value.astype(BF16)
        om[i, h, 0:1, :] = best
        om[i, h, 1:2, :] = weight
        for one in gift(i, h, to):
            go(one)

    def gift_wait(i, h):
        for one in gift(i, h, 0):
            one.wait_recv()

    with jax.named_scope("forward4"):
        for n in range(2):
            kv_wait(at_z(4), n)
    with jax.named_scope("give2"):
        todo = [(at_z(4), 2, 0), (None, 2, 0), (at_z(4), 2, 1), (None, 2, 1)]
        work(todo, {1: lambda: give(2, 0, 2, 1), 3: lambda: give(2, 1, 2, 3)})
    with jax.named_scope("wo2"):
        wo_arrive(left, 1)
        go(wo_pair(wo, wo_pair_send, wo_pair_recv, left, 1, s, partner))
        wo_arrive(right, 0)
        go(wo_pair(wo, wo_pair_send, wo_pair_recv, right, 2, s, partner))

    def side(d, h):
        return entries(both(3, d) + [(at_z(4), d)], (h,), d)

    with jax.named_scope("give31"):
        work(
            side(3, 0) + side(1, 1),
            {3: lambda: give(1, 0, 3, 3), 7: lambda: give(0, 1, 1, 1)},
        )
        work(side(3, 1) + side(1, 0))
    with jax.named_scope("fwait"):
        gift_wait(2, 1)
        give(1, 1, 3, 3, (2,))
        gift_wait(2, 0)
        give(0, 0, 1, 1, (2,))
    with jax.named_scope("last"):
        units(both(1, 0) + both(2, 0) + both(3, 0) + [(at_z(4), 0)], context=0)
    with jax.named_scope("wo3"):
        for n in range(2):
            wo_arrive(over, n)
        go(wo_pair(wo, wo_pair_send, wo_pair_recv, over, 3, s, partner))
    with jax.named_scope("drain"):
        for one in started[:-1]:
            one.wait_send()
        del started[:-1]
    for h in range(heads):
        with jax.named_scope("owait"):
            for i in range(2):
                gift_wait(i, h)
        value, _, _ = merged(0, h, (0, 1))
        att[:, h * head_dim : (h + 1) * head_dim] = value.T.astype(BF16)


def mix_kernel(
    tp_count, att, wo, wo_pair_send, wo_pair_recv, lat, gate_ref, out_hbm,
    mixed, af, out, a_send, a_recv, out_sem, started
):
    s, t = lax.axis_index("sp"), lax.axis_index("tp")
    y, c = t // 2, t % 2
    y_count = tp_count // 2
    partner = y * 2 + 1 - c
    rows, width = mixed.shape

    def slab(dev):
        return pl.ds(pl.multiple_of(dev * rows, rows), rows)

    order = [((y + j) % y_count) * 2 + k for j in (1, y_count - 1, 2) for k in (c, 1 - c)]
    for dev in [partner] + order[4:] + order[:4]:
        remote(att.at[slab(dev)], af.at[t], a_send.at[0], a_recv.at[t], (s, dev)).start()
    others = af.at[pl.ds(0, tp_count - 1)]
    started.append(remote(others, others, a_send.at[0], a_recv.at[0], (s, t)))
    mixed[...] = jnp.dot(att[slab(t), :], wo[t], preferred_element_type=F32)
    for n, dev in enumerate([partner] + order):
        remote(att.at[slab(dev)], af.at[dev], a_send.at[0], a_recv.at[dev], (s, t)).wait_recv()
        if n % 2 == 0:
            wo_pair(wo, wo_pair_send, wo_pair_recv, dev, 0, s, t).wait_recv()
        mixed[...] = mixed[...] + jnp.dot(af[dev], wo[dev], preferred_element_type=F32)
    stores = []
    for n in range(2):
        at = pl.ds(n * (rows // 2), rows // 2)
        value = mixed[at, :]
        inv = lax.rsqrt(jnp.mean(value * value, axis=-1, keepdims=True) + NORM_EPS)
        out[at, :] = (lat[t, at, :].astype(F32) + gate_ref[...] * (value * inv)).astype(BF16)
        one = pltpu.make_async_copy(out.at[at], out_hbm.at[at], out_sem.at[n])
        one.start()
        stores.append(one)
    for one in started:
        one.wait_send()
    for one in stores:
        one.wait()


def whole_kernel(sp_count, tp_count, x_count, head_dim, lift, counts, *refs):
    (
        cond, cond_1, mw, lat, ctx, wq, wk, wv, qg, kg, freq, wo_hbm,
        out, qb, kb, vb, cb, gate, att, wo, wo_sem, *rest,
    ) = refs
    groups, start = [], 0
    for count in counts:
        groups.append(rest[start : start + count])
        start += count
    links, wo_sems, front_scratch, middle_scratch, last_scratch = groups
    lat_all = front_scratch[1]
    started, context_rows = front_kernel(
        sp_count, tp_count, x_count, head_dim, cond, cond_1, mw, lat, ctx, wq, wk, wv, qg, kg, freq,
        qb, kb, vb, cb, gate, *links, *front_scratch, wo_hbm, wo, wo_sem, *wo_sems,
    )
    with jax.named_scope("attn"):
        attend_kernel(
            sp_count, x_count, lift, tp_count, qb, kb, vb, cb, *links, wo, *wo_sems,
            att, *middle_scratch, started, context_rows,
        )
    with jax.named_scope("mix"):
        mix_kernel(tp_count, att, wo, *wo_sems[2:], lat_all, gate, out, *last_scratch, started)


ANY = pl.BlockSpec(memory_space=pl.ANY)
DMA = pltpu.SemaphoreType.DMA


def body(
    latents,
    context,
    cond,
    ctx_cond,
    mod_weight,
    query_weight,
    key_matrix,
    value_matrix,
    out_weight,
    query_gain,
    key_gain,
):
    sp_count, tp_count = lax.axis_size("sp"), lax.axis_size("tp")
    x_count = row_size(sp_count)
    rows, width = latents.shape
    ctx_rows = context.shape[0]
    head_dim = query_gain.shape[0]
    heads = query_weight.shape[1] // head_dim
    all_rows = rows * tp_count
    mod_cols = mod_weight.shape[1]
    quarter = head_dim // 4
    freq = np.float32(ROPE_BASE) ** (-np.arange(quarter, dtype=np.float32) / np.float32(quarter))
    freq = jnp.asarray(freq[:, None], F32)
    lift = math.log(sp_count * all_rows / (2.0 * sp_count * ctx_rows))
    y_count = tp_count // 2
    far = max(y_count - 1, 1)
    z_count = sp_count // x_count
    shared = [
        pltpu.VMEM((x_count, heads, head_dim, all_rows), BF16),
        pltpu.VMEM((z_count, all_rows, head_dim), BF16),
        pltpu.VMEM((z_count, 2, head_dim, all_rows // 2), BF16),
        pltpu.VMEM((z_count, 2, ctx_rows, head_dim), BF16),
        pltpu.VMEM((1, width), F32),
        pltpu.VMEM((all_rows, heads * head_dim), BF16),
        pltpu.VMEM((tp_count, *out_weight.shape), BF16),
        DMA((1,)),
    ]
    wo_sems = [DMA((6,)), DMA((y_count, 2)), DMA((4,)), DMA((y_count,))]
    links = [
        DMA((x_count,)),
        DMA((x_count,)),
        DMA((4, 2, 2)),
        DMA((z_count, 2)),
        DMA((1,)),
        DMA((1,)),
    ]
    front = [
        pltpu.VMEM(mod_weight.shape, F32),
        pltpu.VMEM((tp_count, rows, width), BF16),
        pltpu.VMEM(query_weight.shape, BF16),
        pltpu.VMEM(key_matrix.shape, BF16),
        pltpu.VMEM(value_matrix.shape, BF16),
        pltpu.VMEM((sp_count, 2, mod_cols), F32),
        pltpu.VMEM((tp_count, 2, mod_cols), F32),
        pltpu.VMEM((2, mod_cols * tp_count), F32),
        pltpu.VMEM((4 * rows, width), BF16),
        pltpu.VMEM((ctx_rows, width), BF16),
        pltpu.VMEM((2, quarter, all_rows), F32),
        pltpu.VMEM((2, quarter, all_rows), F32),
        pltpu.VMEM((1, cond.shape[0]), F32),
        pltpu.VMEM((1, cond.shape[0]), F32),
        pltpu.VMEM((1, head_dim), F32),
        pltpu.VMEM((1, head_dim), F32),
        pltpu.VMEM((quarter, 1), F32),
        DMA((11,)),
        DMA((6,)),
        DMA((y_count, 2)),
        DMA((4,)),
        DMA((y_count,)),
        DMA((1,)),
        DMA((1,)),
        DMA((1,)),
        DMA((1,)),
    ]
    far = x_count - 1
    middle = [
        pltpu.VMEM((x_count * heads, 1, all_rows), F32),
        pltpu.VMEM((x_count * heads, 1, all_rows), F32),
        pltpu.VMEM((x_count * heads, head_dim, all_rows), F32),
        pltpu.VMEM((far, heads, head_dim, all_rows), BF16),
        pltpu.VMEM((far, heads, head_dim, all_rows), BF16),
        pltpu.VMEM((far, heads, 2, all_rows), F32),
        pltpu.VMEM((far, heads, 2, all_rows), F32),
        DMA((far, heads)),
        DMA((far, heads)),
        DMA((far, heads)),
        DMA((far, heads)),
    ]
    last = [
        pltpu.VMEM((rows, width), F32),
        pltpu.VMEM((tp_count, rows, heads * head_dim), BF16),
        pltpu.VMEM((rows, width), BF16),
        DMA((1,)),
        DMA((tp_count,)),
        DMA((2,)),
    ]
    groups = (links, wo_sems, front, middle, last)
    counts = tuple(len(one) for one in groups)
    return pl.pallas_call(
        functools.partial(
            whole_kernel, sp_count, tp_count, x_count, head_dim, lift, counts
        ),
        out_shape=jax.ShapeDtypeStruct((rows, width), BF16),
        in_specs=[ANY] * 12,
        out_specs=ANY,
        scratch_shapes=shared + sum(groups, []),
        compiler_params=pltpu.CompilerParams(
            collective_id=0, has_side_effects=True, vmem_limit_bytes=VMEM_BYTES,
        ),
        name="whole",
    )(
        cond[None], ctx_cond[None], mod_weight, latents, context, query_weight, key_matrix, value_matrix,
        query_gain[None], key_gain[None], freq, out_weight,
    )


def solution(mesh):
    placed = (
        P(("sp", "tp"), None),
        P("sp", None),
        P("sp"),
        P("sp"),
        P("sp", "tp"),
        P(None, "tp"),
        P(None, "tp"),
        P(None, "tp"),
        P("tp", None),
        P(),
        P(),
    )
    return jax.shard_map(
        body, mesh=mesh, in_specs=placed, out_specs=P(("sp", "tp"), None), check_vma=False
    )
```

```python
import functools
import math

import jax
import jax.numpy as jnp
import numpy as np
from jax import lax
from jax.experimental import pallas as pl
from jax.experimental.pallas import tpu as pltpu
from jax.sharding import PartitionSpec as P

GRID_W = 64
NORM_EPS = 1e-06
ROPE_BASE = 10000.0
MESH = pl.DeviceIdType.MESH
BF16 = jnp.bfloat16
F32 = jnp.float32
VMEM_BYTES = 67043328


def row_size(sp_count):
    size = 1
    while 4 * size * size <= sp_count:
        size *= 2
    return size


def remote(src, dst, send, recv, dev):
    return pltpu.make_async_remote_copy(
        src_ref=src, dst_ref=dst, send_sem=send, recv_sem=recv, device_id=dev, device_id_type=MESH
    )


def front_kernel(
    sp_count, tp_count, x_count, head_dim,
    cond_hbm, cond_1_hbm, mw_hbm, lat_hbm, ctx_hbm, wq_hbm, wk_hbm, wv_hbm, qg_hbm, kg_hbm, freq_hbm,
    qb, kb, vb, cb, gate_ref, q_send, q_recv, kv_send, kv_recv, c_send, c_recv,
    mw, lat, wq, wk, wv, part, side, tot, mod, xn, ctx, cos_ref, sin_ref,
    cond_ref, cond_1_ref, qg_ref, kg_ref, freq_ref, load_sem,
    lat_send, lat_recv, pair_send, pair_recv, part_send, part_recv, tot_send, tot_recv,
    wo_hbm, wo, wo_sem, wo_send, wo_recv, wo_pair_send, wo_pair_recv,
):
    s, t = lax.axis_index("sp"), lax.axis_index("tp")
    y, c = t // 2, t % 2
    z, x = s // x_count, s % x_count
    z_count = sp_count // x_count
    y_count = tp_count // 2
    partner = y * 2 + 1 - c
    rows = lat.shape[1]
    half = rows // 2
    width = lat.shape[2]
    model_cols = mod.shape[1]
    right, left, far = [((y + j) % y_count) * 2 + c for j in (1, y_count - 1, 2)]

    loads = [
        pltpu.make_async_copy(a, b, load_sem.at[i])
        for i, (a, b) in enumerate(
            (
                (cond_hbm, cond_ref), (cond_1_hbm, cond_1_ref), (mw_hbm, mw), (lat_hbm, lat.at[t]),
                (freq_hbm, freq_ref), (kg_hbm, kg_ref), (qg_hbm, qg_ref), (ctx_hbm, ctx),
                (wk_hbm, wk), (wv_hbm, wv), (wq_hbm, wq),
            )
        )
    ]
    for one in loads[:4]:
        one.start()

    barrier = pltpu.get_barrier_semaphore()
    line = [((z + j) % z_count) * x_count + x for j in range(1, z_count)]
    row = [z * x_count + (x + j) % x_count for j in range(1, x_count)]
    for peer in line + row:
        pl.semaphore_signal(barrier, inc=1, device_id=(peer, t), device_id_type=MESH)
    for j in range(1, tp_count):
        pl.semaphore_signal(barrier, inc=1, device_id=(s, (t + j) % tp_count), device_id_type=MESH)

    for one in loads[4:]:
        one.start()
    wo_load = pltpu.make_async_copy(wo_hbm, wo.at[t], wo_sem.at[0])
    wo_load.start()
    for one in loads[:3]:
        one.wait()
    lines = lax.broadcasted_iota(jnp.int32, (8, cond_ref.shape[1]), 0)
    cond = jnp.where(lines == 0, cond_ref[...], jnp.where(lines == 1, cond_1_ref[...], 0.0))
    cond = cond * jax.nn.sigmoid(cond)
    part[z] = jnp.dot(
        cond, mw[...], precision=lax.Precision.HIGHEST, preferred_element_type=F32
    )[:2]
    loads[3].wait()
    with jax.named_scope("barrier"):
        pl.semaphore_wait(barrier, z_count + x_count + tp_count - 3)

    started = []

    def go(one):
        one.start()
        started.append(one)

    def lat_half(src, n, send, dev):
        at = pl.ds(n * half, half)
        return remote(
            lat.at[src, at], lat.at[src, at], lat_send.at[send], lat_recv.at[src // 2, n], (s, dev)
        )

    def pair(src, send):
        return remote(lat.at[src], lat.at[src], pair_send.at[send], pair_recv.at[src // 2], (s, partner))

    for peer in line:
        remote(part.at[z], part.at[z], part_send.at[0], part_recv.at[0], (peer, t)).start()
    others = part.at[pl.ds(0, z_count - 1)]
    sent_part = remote(others, others, part_send.at[0], part_recv.at[0], (s, t))
    started.append(sent_part)
    go(lat_half(t, 0, 0, right))
    go(lat_half(t, 1, 1, left))
    go(lat_half(t, 1, 2, right))
    go(lat_half(t, 0, 3, left))
    go(pair(t, 0))

    loads[4].wait()
    where = s * cos_ref.shape[2] + lax.broadcasted_iota(jnp.int32, cos_ref.shape[1:], 1)
    for n, place in enumerate((where // GRID_W, where % GRID_W)):
        angle = place.astype(F32) * freq_ref[...]
        cos_ref[n] = jnp.cos(angle)
        sin_ref[n] = jnp.sin(angle)

    with jax.named_scope("modsum"):
        sent_part.wait_recv()
        total = part[0]
        for j in range(1, z_count):
            total = total + part[j]
        side[x] = total
        for peer in row:
            remote(side.at[x], side.at[x], part_send.at[1], part_recv.at[1], (peer, t)).start()
        others = side.at[pl.ds(0, x_count - 1)]
        sent_side = remote(others, others, part_send.at[1], part_recv.at[1], (s, t))
        started.append(sent_side)
        sent_side.wait_recv()
        total = side[0]
        for j in range(1, x_count):
            total = total + side[j]
        tot[t] = total
    for j in range(1, tp_count):
        remote(tot.at[t], tot.at[t], tot_send.at[0], tot_recv.at[0], (s, (t + j) % tp_count)).start()

    others = tot.at[pl.ds(0, tp_count - 1)]
    sent_tot = remote(others, others, tot_send.at[0], tot_recv.at[0], (s, t))
    started.append(sent_tot)

    with jax.named_scope("latwait"):
        lat_half(left, 0, 0, t).wait_recv()
        go(lat_half(left, 0, 4, right))
        lat_half(right, 1, 0, t).wait_recv()
        go(lat_half(right, 1, 5, left))
        lat_half(left, 1, 0, t).wait_recv()
        go(pair(left, 1))
        lat_half(right, 0, 0, t).wait_recv()
        go(pair(right, 2))

    with jax.named_scope("totwait"):
        sent_tot.wait_recv()
    cols = model_cols // tp_count
    for j in range(tp_count):
        mod[:, j * cols : (j + 1) * cols] = tot[j]
    gate_ref[...] = mod[0:1, 2 * width :]

    def modulate(x_rows, r):
        x_rows = x_rows.astype(F32)
        scaled = x_rows * lax.rsqrt(jnp.mean(x_rows * x_rows, axis=-1, keepdims=True) + NORM_EPS)
        shift, scale = mod[r : r + 1, :width], mod[r : r + 1, width : 2 * width]
        return (scaled * (1.0 + scale) + shift).astype(BF16)

    with jax.named_scope("loadwait"):
        for one in loads[5:]:
            one.wait()

    q4 = head_dim // 4
    qgain, kgain = qg_ref[...], kg_ref[...]

    def turn(yt, cos, sin):
        out = []
        for n in range(2):
            a = yt[2 * n * q4 : (2 * n + 1) * q4]
            b = yt[(2 * n + 1) * q4 : (2 * n + 2) * q4]
            out += [a * cos[n] - b * sin[n], b * cos[n] + a * sin[n]]
        return jnp.concatenate(out, axis=0)

    def unit(yh, gain):
        return yh * lax.rsqrt(jnp.mean(yh * yh, axis=-1, keepdims=True) + NORM_EPS) * gain

    span = 2 * rows

    def block(n, places):
        for m, yy in enumerate(places):
            for i in range(2):
                xn[(2 * m + i) * rows : (2 * m + i + 1) * rows, :] = modulate(lat[yy * 2 + i], 0)
        spots = [pl.ds(pl.multiple_of(yy * span, span), span) for yy in places]
        turns = [(cos_ref[:, :, at], sin_ref[:, :, at]) for at in spots]
        key = unit(jnp.dot(xn[...], wk[...], preferred_element_type=F32), kgain)
        val = jnp.dot(xn[...], wv[...], preferred_element_type=F32)
        for m in range(2):
            at = slice((2 * n + m) * span, (2 * n + m + 1) * span)
            kb[z, at, :] = turn(key[m * span : (m + 1) * span].T, *turns[m]).T.astype(BF16)
        vb[z, n] = val.T.astype(BF16)
        for way, dz in ((0, 1), (1, z_count - 1)):
            peer = ((z + dz) % z_count) * x_count + x
            copies, all_sent = kv_copy(kb, vb, kv_send, kv_recv, z, n, 0, way, peer, t)
            for one in copies:
                one.start()
            started.append(all_sent)
        full = jnp.dot(xn[...], wq[...], preferred_element_type=F32)
        for m in range(2):
            for h in range(full.shape[1] // head_dim):
                yh = unit(full[m * span : (m + 1) * span, h * head_dim : (h + 1) * head_dim], qgain)
                qb[x, h, :, spots[m]] = turn(yh.T, *turns[m]).astype(BF16)
            for d in (1, x_count - 1):
                peer = z * x_count + (x + d) % x_count
                q_copy(qb, q_send, q_recv, x, places[m], d, peer, t).start()

    def pair_wait(yy):
        other = yy * 2 + 1 - c
        remote(lat.at[other], lat.at[other], pair_send.at[0], pair_recv.at[yy], (s, t)).wait_recv()

    def context_rows():
        cn = modulate(ctx[...], 1)
        kc = jnp.dot(cn, wk[...], preferred_element_type=F32)
        vc = jnp.dot(cn, wv[...], preferred_element_type=F32)
        cb[z, 0] = unit(kc, kgain).astype(BF16)
        cb[z, 1] = vc.astype(BF16)
        for j in range(1, z_count):
            remote(
                cb.at[z], cb.at[z], c_send.at[0], c_recv.at[0], (((z + j) % z_count) * x_count + x, t)
            ).start()
        others = cb.at[pl.ds(0, z_count - 1)]
        started.append(remote(others, others, c_send.at[0], c_recv.at[0], (s, t)))

    spots_y = [(y + step) % y_count for step in (0, 1, y_count - 1, 2)]
    with jax.named_scope("far"):
        lat_half(far, 0, 0, t).wait_recv()
        lat_half(far, 1, 0, t).wait_recv()
        go(pair(far, 3))
        pair_wait(spots_y[0])
        pair_wait(spots_y[1])
    wo_load.wait()
    for src, n, send, dev in ((t, 0, 0, right), (t, 1, 1, left), (t, 1, 2, right), (t, 0, 3, left)):
        go(wo_half(wo, wo_send, wo_recv, src, n, send, s, dev))
    go(wo_pair(wo, wo_pair_send, wo_pair_recv, t, 0, s, partner))
    with jax.named_scope("block"):
        block(0, spots_y[:2])
    with jax.named_scope("far"):
        pair_wait(spots_y[2])
        pair_wait(spots_y[3])
    with jax.named_scope("block"):
        block(1, spots_y[2:])
    for yy in spots_y:
        q_copy(qb, q_send, q_recv, x, yy, 2, z * x_count + (x + 2) % x_count, t).start()
    for d in range(1, x_count):
        started.append(remote(qb.at[x], qb.at[x], q_send.at[d], q_recv.at[x], (s, t)))
    return started, context_rows


def wo_half(wo, wo_send, wo_recv, src, n, send, s, dev):
    half = wo.shape[1] // 2
    ref = wo.at[src, pl.ds(n * half, half)]
    return remote(ref, ref, wo_send.at[send], wo_recv.at[src // 2, n], (s, dev))


def wo_pair(wo, send_sem, recv_sem, src, send, s, dev):
    return remote(wo.at[src], wo.at[src], send_sem.at[send], recv_sem.at[src // 2], (s, dev))


def kv_copy(kb, vb, kv_send, kv_recv, src, n, hop, way, peer, t, which=(0, 1)):
    half = kb.shape[1] // 2
    key = kb.at[src, pl.ds(n * half, half)]
    refs = [(key, vb.at[src, n])[i] for i in which]
    both = [
        remote(ref, ref, kv_send.at[hop, way, n], kv_recv.at[src, n], (peer, t)) for ref in refs
    ]
    whole = kb.at[src] if len(which) == 2 else key
    return both, remote(whole, whole, kv_send.at[hop, way, n], kv_recv.at[src, n], (peer, t))


def q_copy(qb, q_send, q_recv, owner, yy, d, peer, t):
    span = qb.shape[3] // 4
    at = pl.ds(pl.multiple_of(yy * span, span), span)
    ref = qb.at[owner, :, :, at]
    return remote(ref, ref, q_send.at[d], q_recv.at[owner], (peer, t))


def attend_kernel(
    sp_count, x_count, lift,
    tp_count, qb, kb, vb, cb, q_send, q_recv, kv_send, kv_recv, c_send, c_recv,
    wo, wo_send, wo_recv, wo_pair_send, wo_pair_recv,
    att, top, tot, acc, ob, ib, om, im, o_send, o_recv, m_send, m_recv, started, context_rows,
):
    s, t = lax.axis_index("sp"), lax.axis_index("tp")
    z, x = s // x_count, s % x_count
    z_count = sp_count // x_count
    heads, head_dim, rows = qb.shape[1:]
    factor = head_dim ** (-0.5) * math.log2(math.e)
    bias = lift * head_dim**0.5

    top[...] = jnp.full_like(top, -1e30)
    tot[...] = jnp.zeros_like(tot)
    acc[...] = jnp.zeros_like(acc)

    y, c = t // 2, t % 2
    y_count = tp_count // 2
    partner = y * 2 + 1 - c
    right, left, over = [((y + j) % y_count) * 2 + c for j in (1, y_count - 1, 2)]

    def wo_arrive(src, n):
        wo_half(wo, wo_send, wo_recv, src, n, 0, s, t).wait_recv()

    def go(one):
        one.start()
        started.append(one)

    def at_z(k):
        return (z + k + z_count) % z_count

    def soft(d, h, sc, values):
        i = d * heads + h
        old = top[i]
        new = jnp.maximum(old, jnp.max(sc, axis=0, keepdims=True))
        p = jnp.exp2((sc - new) * factor)
        f = jnp.exp2((old - new) * factor)
        top[i] = new
        tot[i] = tot[i] * f + jnp.sum(p, axis=0, keepdims=True)
        p = p.astype(BF16)
        new_acc = acc[i] * f
        step = p.shape[0] // len(values)
        for n, one in enumerate(values):
            new_acc = new_acc + jnp.dot(one, p[n * step : (n + 1) * step], preferred_element_type=F32)
        acc[i] = new_acc

    def entries(pairs, hs=(0, 1), context=None):
        todo = [(kv, d, h) for kv, d in pairs for h in hs]
        return todo + ([] if context is None else [(None, context, h) for h in hs])

    def units(pairs, context=None):
        work(entries(pairs, context=context))

    def work(todo, then={}):
        if any(one[0] is None for one in todo):
            ckeys = jnp.concatenate([cb[j, 0] for j in range(z_count)], axis=0)
            cvals = jnp.concatenate([cb[j, 1] for j in range(z_count)], axis=0)
            cvals = cvals.astype(F32).T.astype(BF16)

        def scores(one):
            kv, d, h = one
            query = qb[(x + d) % x_count, h]
            if kv is None:
                return jnp.dot(ckeys, query, preferred_element_type=F32) + bias
            return jnp.dot(kb[kv], query, preferred_element_type=F32)

        ahead = [scores(one) for one in todo[:2]]
        for n, one in enumerate(todo):
            sc = ahead.pop(0)
            if n + 2 < len(todo):
                ahead.append(scores(todo[n + 2]))
            kv, d, h = one
            soft(d, h, sc, [cvals] if kv is None else [vb[kv, 0], vb[kv, 1]])
            if n in then:
                then[n]()

    def kv_wait(src, n):
        kv_copy(kb, vb, kv_send, kv_recv, src, n, 0, 0, s, t)[1].wait_recv()

    def forward(k, n, which_r=(0, 1), which_l=(0, 1)):
        for sign, way, which in ((-1, 0, which_r), (1, 1, which_l)):
            src = at_z(sign * k)
            kv_wait(src, n)
            peer = at_z(1 if way == 0 else -1) * x_count + x
            copies, all_sent = kv_copy(kb, vb, kv_send, kv_recv, src, n, k, way, peer, t, which)
            for one in copies:
                one.start()
            started.append(all_sent)

    def q_arrive(d):
        owner = (x + d) % x_count
        remote(qb.at[owner], qb.at[owner], q_send.at[0], q_recv.at[owner], (s, t)).wait_recv()

    def both(k, d):
        return [(at_z(-k), d), (at_z(k), d)]

    with jax.named_scope("own"):
        units([(z, 0)])
    with jax.named_scope("context"):
        context_rows()
    with jax.named_scope("forward1"):
        forward(1, 0)
        forward(1, 1)
    with jax.named_scope("q1"):
        q_arrive(3)
        q_arrive(1)
    with jax.named_scope("units1"):
        units([(z, 3), (z, 1)] + both(1, 3))
    with jax.named_scope("forward2"):
        forward(2, 0)
    with jax.named_scope("units2"):
        units(both(1, 1) + both(1, 0))
    with jax.named_scope("forward2"):
        forward(2, 1)
    with jax.named_scope("wo1"):
        wo_arrive(left, 0)
        go(wo_half(wo, wo_send, wo_recv, left, 0, 4, s, right))
        wo_arrive(right, 1)
        go(wo_half(wo, wo_send, wo_recv, right, 1, 5, s, left))
    with jax.named_scope("q2"):
        q_arrive(2)
    with jax.named_scope("units3"):
        units([(z, 2)] + both(1, 2))
    with jax.named_scope("forward3"):
        forward(3, 0, (0,), (1,))
    with jax.named_scope("units4"):
        units(both(2, 2) + both(2, 3))
    with jax.named_scope("forward3"):
        forward(3, 1, (0,), (1,))
    with jax.named_scope("units5"):
        units(both(2, 1) + both(3, 2))
    others = cb.at[pl.ds(0, z_count - 1)]
    remote(others, others, c_send.at[0], c_recv.at[0], (s, t)).wait_recv()

    def gift(i, h, d):
        peer = z * x_count + (x + d) % x_count
        return [
            remote(a.at[i, h], b.at[i, h], u.at[i, h], v.at[i, h], (peer, t))
            for a, b, u, v in ((om, im, m_send, m_recv), (ob, ib, o_send, o_recv))
        ]

    def merged(i, h, parts):
        best = top[i * heads + h]
        for part in parts:
            best = jnp.maximum(best, im[part, h, 0:1, :])
        f = jnp.exp2((top[i * heads + h] - best) * factor)
        value, weight = acc[i * heads + h] * f, tot[i * heads + h] * f
        for part in parts:
            w = im[part, h, 1:2, :] * jnp.exp2((im[part, h, 0:1, :] - best) * factor)
            value = value + ib[part, h].astype(F32) * w
            weight = weight + w
        return value / weight, best, weight

    def give(i, h, d, to, parts=()):
        value, best, weight = merged(d, h, parts)
        ob[i, h] = value.astype(BF16)
        om[i, h, 0:1, :] = best
        om[i, h, 1:2, :] = weight
        for one in gift(i, h, to):
            go(one)

    def gift_wait(i, h):
        for one in gift(i, h, 0):
            one.wait_recv()

    with jax.named_scope("forward4"):
        for n in range(2):
            kv_wait(at_z(4), n)
    with jax.named_scope("give2"):
        todo = [(at_z(4), 2, 0), (None, 2, 0), (at_z(4), 2, 1), (None, 2, 1)]
        work(todo, {1: lambda: give(2, 0, 2, 1), 3: lambda: give(2, 1, 2, 3)})
    with jax.named_scope("wo2"):
        wo_arrive(left, 1)
        go(wo_pair(wo, wo_pair_send, wo_pair_recv, left, 1, s, partner))
        wo_arrive(right, 0)
        go(wo_pair(wo, wo_pair_send, wo_pair_recv, right, 2, s, partner))

    def side(d, h):
        return entries(both(3, d) + [(at_z(4), d)], (h,), d)

    with jax.named_scope("give31"):
        work(
            side(3, 0) + side(1, 1),
            {3: lambda: give(1, 0, 3, 3), 7: lambda: give(0, 1, 1, 1)},
        )
        work(side(3, 1) + side(1, 0))
    with jax.named_scope("fwait"):
        gift_wait(2, 1)
        give(1, 1, 3, 3, (2,))
        gift_wait(2, 0)
        give(0, 0, 1, 1, (2,))
    with jax.named_scope("last"):
        units(both(2, 0) + both(3, 0) + [(at_z(4), 0)], context=0)
    with jax.named_scope("wo3"):
        for n in range(2):
            wo_arrive(over, n)
        go(wo_pair(wo, wo_pair_send, wo_pair_recv, over, 3, s, partner))
    with jax.named_scope("drain"):
        for one in started[:-1]:
            one.wait_send()
        del started[:-1]
    for h in range(heads):
        with jax.named_scope("owait"):
            for i in range(2):
                gift_wait(i, h)
        value, _, _ = merged(0, h, (0, 1))
        att[:, h * head_dim : (h + 1) * head_dim] = value.T.astype(BF16)


def mix_kernel(
    tp_count, att, wo, wo_pair_send, wo_pair_recv, lat, gate_ref, out_hbm,
    mixed, af, out, a_send, a_recv, out_sem, started
):
    s, t = lax.axis_index("sp"), lax.axis_index("tp")
    y, c = t // 2, t % 2
    y_count = tp_count // 2
    partner = y * 2 + 1 - c
    rows, width = mixed.shape

    def slab(dev):
        return pl.ds(pl.multiple_of(dev * rows, rows), rows)

    order = [((y + j) % y_count) * 2 + k for j in (1, y_count - 1, 2) for k in (c, 1 - c)]
    for dev in [partner] + order[4:] + order[:4]:
        remote(att.at[slab(dev)], af.at[t], a_send.at[0], a_recv.at[t], (s, dev)).start()
    others = af.at[pl.ds(0, tp_count - 1)]
    started.append(remote(others, others, a_send.at[0], a_recv.at[0], (s, t)))
    mixed[...] = jnp.dot(att[slab(t), :], wo[t], preferred_element_type=F32)
    for n, dev in enumerate([partner] + order):
        remote(att.at[slab(dev)], af.at[dev], a_send.at[0], a_recv.at[dev], (s, t)).wait_recv()
        if n % 2 == 0:
            wo_pair(wo, wo_pair_send, wo_pair_recv, dev, 0, s, t).wait_recv()
        mixed[...] = mixed[...] + jnp.dot(af[dev], wo[dev], preferred_element_type=F32)
    stores = []
    for n in range(2):
        at = pl.ds(n * (rows // 2), rows // 2)
        value = mixed[at, :]
        inv = lax.rsqrt(jnp.mean(value * value, axis=-1, keepdims=True) + NORM_EPS)
        out[at, :] = (lat[t, at, :].astype(F32) + gate_ref[...] * (value * inv)).astype(BF16)
        one = pltpu.make_async_copy(out.at[at], out_hbm.at[at], out_sem.at[n])
        one.start()
        stores.append(one)
    for one in started:
        one.wait_send()
    for one in stores:
        one.wait()


def whole_kernel(sp_count, tp_count, x_count, head_dim, lift, counts, *refs):
    (
        cond, cond_1, mw, lat, ctx, wq, wk, wv, qg, kg, freq, wo_hbm,
        out, qb, kb, vb, cb, gate, att, wo, wo_sem, *rest,
    ) = refs
    groups, start = [], 0
    for count in counts:
        groups.append(rest[start : start + count])
        start += count
    links, wo_sems, front_scratch, middle_scratch, last_scratch = groups
    lat_all = front_scratch[1]
    started, context_rows = front_kernel(
        sp_count, tp_count, x_count, head_dim, cond, cond_1, mw, lat, ctx, wq, wk, wv, qg, kg, freq,
        qb, kb, vb, cb, gate, *links, *front_scratch, wo_hbm, wo, wo_sem, *wo_sems,
    )
    with jax.named_scope("attn"):
        attend_kernel(
            sp_count, x_count, lift, tp_count, qb, kb, vb, cb, *links, wo, *wo_sems,
            att, *middle_scratch, started, context_rows,
        )
    with jax.named_scope("mix"):
        mix_kernel(tp_count, att, wo, *wo_sems[2:], lat_all, gate, out, *last_scratch, started)


ANY = pl.BlockSpec(memory_space=pl.ANY)
DMA = pltpu.SemaphoreType.DMA


def body(
    latents,
    context,
    cond,
    ctx_cond,
    mod_weight,
    query_weight,
    key_matrix,
    value_matrix,
    out_weight,
    query_gain,
    key_gain,
):
    sp_count, tp_count = lax.axis_size("sp"), lax.axis_size("tp")
    x_count = row_size(sp_count)
    rows, width = latents.shape
    ctx_rows = context.shape[0]
    head_dim = query_gain.shape[0]
    heads = query_weight.shape[1] // head_dim
    all_rows = rows * tp_count
    mod_cols = mod_weight.shape[1]
    quarter = head_dim // 4
    freq = np.float32(ROPE_BASE) ** (-np.arange(quarter, dtype=np.float32) / np.float32(quarter))
    freq = jnp.asarray(freq[:, None], F32)
    lift = math.log(sp_count * all_rows / (2.0 * sp_count * ctx_rows))
    y_count = tp_count // 2
    far = max(y_count - 1, 1)
    z_count = sp_count // x_count
    shared = [
        pltpu.VMEM((x_count, heads, head_dim, all_rows), BF16),
        pltpu.VMEM((z_count, all_rows, head_dim), BF16),
        pltpu.VMEM((z_count, 2, head_dim, all_rows // 2), BF16),
        pltpu.VMEM((z_count, 2, ctx_rows, head_dim), BF16),
        pltpu.VMEM((1, width), F32),
        pltpu.VMEM((all_rows, heads * head_dim), BF16),
        pltpu.VMEM((tp_count, *out_weight.shape), BF16),
        DMA((1,)),
    ]
    wo_sems = [DMA((6,)), DMA((y_count, 2)), DMA((4,)), DMA((y_count,))]
    links = [
        DMA((x_count,)),
        DMA((x_count,)),
        DMA((4, 2, 2)),
        DMA((z_count, 2)),
        DMA((1,)),
        DMA((1,)),
    ]
    front = [
        pltpu.VMEM(mod_weight.shape, F32),
        pltpu.VMEM((tp_count, rows, width), BF16),
        pltpu.VMEM(query_weight.shape, BF16),
        pltpu.VMEM(key_matrix.shape, BF16),
        pltpu.VMEM(value_matrix.shape, BF16),
        pltpu.VMEM((z_count, 2, mod_cols), F32),
        pltpu.VMEM((x_count, 2, mod_cols), F32),
        pltpu.VMEM((tp_count, 2, mod_cols), F32),
        pltpu.VMEM((2, mod_cols * tp_count), F32),
        pltpu.VMEM((4 * rows, width), BF16),
        pltpu.VMEM((ctx_rows, width), BF16),
        pltpu.VMEM((2, quarter, all_rows), F32),
        pltpu.VMEM((2, quarter, all_rows), F32),
        pltpu.VMEM((1, cond.shape[0]), F32),
        pltpu.VMEM((1, cond.shape[0]), F32),
        pltpu.VMEM((1, head_dim), F32),
        pltpu.VMEM((1, head_dim), F32),
        pltpu.VMEM((quarter, 1), F32),
        DMA((11,)),
        DMA((6,)),
        DMA((y_count, 2)),
        DMA((4,)),
        DMA((y_count,)),
        DMA((2,)),
        DMA((2,)),
        DMA((1,)),
        DMA((1,)),
    ]
    far = x_count - 1
    middle = [
        pltpu.VMEM((x_count * heads, 1, all_rows), F32),
        pltpu.VMEM((x_count * heads, 1, all_rows), F32),
        pltpu.VMEM((x_count * heads, head_dim, all_rows), F32),
        pltpu.VMEM((far, heads, head_dim, all_rows), BF16),
        pltpu.VMEM((far, heads, head_dim, all_rows), BF16),
        pltpu.VMEM((far, heads, 2, all_rows), F32),
        pltpu.VMEM((far, heads, 2, all_rows), F32),
        DMA((far, heads)),
        DMA((far, heads)),
        DMA((far, heads)),
        DMA((far, heads)),
    ]
    last = [
        pltpu.VMEM((rows, width), F32),
        pltpu.VMEM((tp_count, rows, heads * head_dim), BF16),
        pltpu.VMEM((rows, width), BF16),
        DMA((1,)),
        DMA((tp_count,)),
        DMA((2,)),
    ]
    groups = (links, wo_sems, front, middle, last)
    counts = tuple(len(one) for one in groups)
    return pl.pallas_call(
        functools.partial(
            whole_kernel, sp_count, tp_count, x_count, head_dim, lift, counts
        ),
        out_shape=jax.ShapeDtypeStruct((rows, width), BF16),
        in_specs=[ANY] * 12,
        out_specs=ANY,
        scratch_shapes=shared + sum(groups, []),
        compiler_params=pltpu.CompilerParams(
            collective_id=0, has_side_effects=True, vmem_limit_bytes=VMEM_BYTES,
        ),
        name="whole",
    )(
        cond[None], ctx_cond[None], mod_weight, latents, context, query_weight, key_matrix, value_matrix,
        query_gain[None], key_gain[None], freq, out_weight,
    )


def solution(mesh):
    placed = (
        P(("sp", "tp"), None),
        P("sp", None),
        P("sp"),
        P("sp"),
        P("sp", "tp"),
        P(None, "tp"),
        P(None, "tp"),
        P(None, "tp"),
        P("tp", None),
        P(),
        P(),
    )
    return jax.shard_map(
        body, mesh=mesh, in_specs=placed, out_specs=P(("sp", "tp"), None), check_vma=False
    )
```
